128 devices in a mesh: sp: 32 (over z, y, core), tp: 4 (over x).
Axes of the slice: x: 4, y: 4, z: 4, core: 2. Of those that a mesh axis runs over, the one named last changes fastest.
Arguments:
- inputs: bfloat16 [16384, 3072], P('sp', 'tp'), may hold values from -6 to 6
- w_query: bfloat16 [3072, 1536], P(None, 'tp'), may hold values from -0.109375 to 0.109375
- w_key: bfloat16 [3072, 1536], P(None, 'tp'), may hold values from -0.109375 to 0.109375
- w_value: bfloat16 [3072, 1536], P(None, 'tp'), may hold values from -0.109375 to 0.109375
- rel_bias: float32 [320, 24], P(None, 'tp'), may hold values from -5 to 254
- d_out: bfloat16 [16384, 1536], P('sp', 'tp'), may hold values from -6 to 6
Outputs:
- grad_inputs: bfloat16 [16384, 3072], P('sp', 'tp')
- grad_w_query: float32 [3072, 1536], P('sp', 'tp')
- grad_w_key: float32 [3072, 1536], P('sp', 'tp')
- grad_w_value: float32 [3072, 1536], P('sp', 'tp')
- grad_bias: float32 [320, 24], P(None, 'tp')
The draws below stay inside these ranges and needn't reach their ends.
All inputs are finite; a program needn't handle non-finite values.
Results may differ from the reference program's by a relative error of at most 0.015.
Values may be sent and summed in bfloat16 or wider, within the bound.
A program may use at most 128 MiB of HBM per device.

```python
import jax
import jax.numpy as jnp
import numpy as np
from jax import lax

D = 3072
HEADS = 24
HEAD = 64
SEG = 64
LEFT = 4
REL_MAX = 256
ATT = 1536
REL_SIZE = 320
TOKENS = 16384
N_TP = 4


def draw_rel_bias(key, part):
    base = jnp.clip(jax.random.normal(key, (REL_SIZE, HEADS), jnp.float32), -5.0, 5.0)
    return base


def spiked(drawn, rng, source, target, parts, factor):
    def block_of(position):
        return (jnp.arange(drawn.shape[position]) // (drawn.shape[position] // parts)).reshape((-1,) + (1,) * (drawn.ndim - 1 - position))

    near = jax.random.permutation(rng, parts)[block_of(target)]
    far = (block_of(target) + parts // 2) % parts
    return jnp.where((block_of(source) == near) | (block_of(source) == far), factor * drawn, drawn)


def levels(key, extent, shards, smallest, largest):
    gain = 1.0
    for axis_at, shards_of in shards:
        steps = jax.random.uniform(jax.random.fold_in(jax.random.fold_in(key, 6), axis_at), (shards_of,), jnp.float32, smallest / len(shards), largest / len(shards))
        gain = gain * jnp.repeat(jnp.exp(steps), extent[axis_at] // shards_of).reshape((-1,) + (1,) * (len(extent) - 1 - axis_at))
    return gain


def noise(own_key, dims, scale, reach, cuts=(), held_as=jnp.bfloat16):
    factor_of = levels(own_key, dims, cuts, -0.22, 0.18) if cuts else 1.0
    entries = jax.random.normal(own_key, dims, jnp.float32) * scale * factor_of
    return jnp.minimum(jnp.maximum(entries, -reach), reach).astype(held_as)


def heavy_noise(own_key, extent, scale, most, split, heavy, held_as=jnp.bfloat16):
    array = scale * jax.random.normal(own_key, extent, jnp.float32)
    if split:
        array = array * levels(own_key, extent, split, -0.22, 0.18)
    return jnp.clip(spiked(array, jax.random.fold_in(own_key, 3), *heavy), -most, most).astype(held_as)


def setup_inputs(seed: int = 0) -> dict:
    keys = jax.random.split(jax.random.key(seed), 7)
    inputs = heavy_noise(keys[0], (TOKENS, D), 1.0, 6.0, ((0, 32), (1, 4)), (0, 1, 32, 2.75))
    w_query = noise(keys[1], (D, ATT), D ** -0.5, 0.109375, ((1, 4),))
    w_key = noise(keys[2], (D, ATT), D ** -0.5, 0.109375, ((1, 4),))
    w_value = noise(keys[3], (D, ATT), D ** -0.5, 0.109375, ((1, 4),))
    rel_bias = draw_rel_bias(jax.random.fold_in(keys[6], 71), 0)
    d_out = noise(keys[5], (TOKENS, ATT), 1.0, 6.0, ((0, 32), (1, 4)))
    return dict(inputs=inputs, w_query=w_query, w_key=w_key, w_value=w_value, rel_bias=rel_bias, d_out=d_out)


def bias_table(rel_bias):
    query_row = np.arange(SEG)[:, None]
    key_row = np.arange((LEFT + 1) * SEG)[None, :]
    distance = np.clip(LEFT * SEG + query_row - key_row, 1 - SEG, REL_MAX) + SEG - 1
    picked = jnp.take(rel_bias, jnp.asarray(distance.astype(np.int32)), axis=0)
    return jnp.transpose(picked, (2, 0, 1))

def banded(source, seg_count):
    pieces = source.reshape((seg_count + LEFT, SEG) + source.shape[1:])
    return jnp.concatenate([pieces[offset_seg:offset_seg + seg_count] for offset_seg in range(LEFT + 1)], axis=1)

def unbanded(band_grads, seg_count):
    pieces = band_grads.reshape((seg_count, LEFT + 1, SEG) + band_grads.shape[2:])
    widths = ((0, 0),) * (pieces.ndim - 3)
    total = jnp.zeros((seg_count + LEFT, SEG) + band_grads.shape[2:], band_grads.dtype)
    for offset_seg in range(LEFT + 1):
        total = total + jnp.pad(pieces[:, offset_seg], ((offset_seg, LEFT - offset_seg), (0, 0)) + widths)
    return total.reshape(((seg_count + LEFT) * SEG,) + band_grads.shape[2:])

def one_head(operands):
    q_head, k_head, v_head, d_head, bias_head = operands
    seg_count = TOKENS // SEG
    score_scale = HEAD ** (-0.5)
    pad_rows = ((LEFT * SEG, 0), (0, 0))
    key_band = banded(jnp.pad(k_head, pad_rows), seg_count).astype(jnp.float32)
    value_band = banded(jnp.pad(v_head, pad_rows), seg_count).astype(jnp.float32)
    q_seg = q_head.reshape(seg_count, SEG, HEAD).astype(jnp.float32)
    d_seg = d_head.reshape(seg_count, SEG, HEAD).astype(jnp.float32)
    scores = jnp.einsum('cqd,ckd->cqk', q_seg, key_band) * score_scale + bias_head[None]
    key_pos = (jnp.arange(seg_count)[:, None] - LEFT) * SEG + jnp.arange((LEFT + 1) * SEG)[None, :]
    scores = jnp.where((key_pos >= 0)[:, None, :], scores, -jnp.inf)
    top = lax.optimization_barrier(jnp.max(scores, axis=-1, keepdims=True))
    lse = top + jnp.log(lax.optimization_barrier(jnp.sum(jnp.exp(scores - top), axis=-1, keepdims=True)))
    prob = jnp.exp(scores - lse)
    prob_low = prob.astype(jnp.bfloat16).astype(jnp.float32)
    attended = jnp.einsum('cqk,ckd->cqd', prob_low, value_band)
    delta = lax.optimization_barrier(jnp.sum(d_seg * attended, axis=-1, keepdims=True))
    grad_prob = jnp.einsum('cqd,ckd->cqk', d_seg, value_band)
    dscore = prob * (grad_prob - delta)
    dscore_low = dscore.astype(jnp.bfloat16).astype(jnp.float32)
    grad_query = jnp.einsum('cqk,ckd->cqd', dscore_low, key_band) * score_scale
    grad_kband = jnp.einsum('cqk,cqd->ckd', dscore_low, q_seg) * score_scale
    grad_vband = jnp.einsum('cqk,cqd->ckd', prob_low, d_seg)
    grad_key = unbanded(grad_kband, seg_count)[LEFT * SEG:]
    grad_value = unbanded(grad_vband, seg_count)[LEFT * SEG:]
    return (grad_query.reshape(TOKENS, HEAD).astype(jnp.bfloat16), grad_key.astype(jnp.bfloat16), grad_value.astype(jnp.bfloat16), lax.optimization_barrier(jnp.sum(dscore, axis=0)))

def reference(inputs, w_query, w_key, w_value, rel_bias, d_out):
    query = jnp.dot(inputs, w_query, preferred_element_type=jnp.float32).astype(jnp.bfloat16)
    key = jnp.dot(inputs, w_key, preferred_element_type=jnp.float32).astype(jnp.bfloat16)
    value = jnp.dot(inputs, w_value, preferred_element_type=jnp.float32).astype(jnp.bfloat16)

    def by_head(matrix):
        return matrix.reshape(TOKENS, HEADS, HEAD).transpose(1, 0, 2)

    def by_token(matrix):
        return matrix.transpose(1, 0, 2).reshape(TOKENS, HEADS * HEAD)
    bias_full, bias_back = jax.vjp(bias_table, rel_bias)
    head_q, head_k, head_v, score_sum = lax.map(one_head, (by_head(query), by_head(key), by_head(value), by_head(d_out), bias_full))
    grad_query = by_token(head_q)
    grad_key = by_token(head_k)
    grad_value = by_token(head_v)
    grad_bias = bias_back(score_sum)[0]
    contract = (((0,), (0,)), ((), ()))
    grad_w_query = lax.dot_general(inputs, grad_query, contract, preferred_element_type=jnp.float32)
    grad_w_key = lax.dot_general(inputs, grad_key, contract, preferred_element_type=jnp.float32)
    grad_w_value = lax.dot_general(inputs, grad_value, contract, preferred_element_type=jnp.float32)
    group = HEADS * HEAD // N_TP
    total = jnp.zeros((TOKENS, D), jnp.float32)
    for index in range(N_TP):
        cols = slice(index * group, (index + 1) * group)
        partial_value = jnp.dot(grad_query[:, cols], w_query[:, cols].T, preferred_element_type=jnp.float32)
        partial_value = partial_value + jnp.dot(grad_key[:, cols], w_key[:, cols].T, preferred_element_type=jnp.float32)
        partial_value = partial_value + jnp.dot(grad_value[:, cols], w_value[:, cols].T, preferred_element_type=jnp.float32)
        rounded = lax.optimization_barrier(partial_value.astype(jnp.bfloat16))
        total = total + rounded.astype(jnp.float32)
    grad_inputs = total.astype(jnp.bfloat16)
    return (grad_inputs, grad_w_query, grad_w_key, grad_w_value, grad_bias)
```

```python
import functools

import jax
import jax.numpy as jnp
from jax import lax
from jax.experimental import pallas as pl
from jax.experimental.pallas import tpu as pltpu
from jax.sharding import Mesh
from jax.sharding import PartitionSpec as P

SP = ("sp_0", "sp_1", "sp_2")
MESH = pl.DeviceIdType.MESH
BF = jnp.bfloat16
F32 = jnp.float32
NSEM = 100

NN = (((1,), (0,)), ((), ()))
NT = (((1,), (1,)), ((), ()))


def dot(a, b, dims=NN):
    return lax.dot_general(a, b, dims, preferred_element_type=F32)


def kernel(
    x_hbm, wq_hbm, wk_hbm, wv_hbm, rb_hbm, do_hbm,
    gx_ref, gw_ref, gb_ref,
    xbuf, w, xt, acc, kext, vext, qs, do, kt, dk_acc, dv_acc, bias, gbias, g,
    hb_send, hb_recv, dwb, crecv, s1,
    fold, recv2, s2, recv3,
    dx_send, dx_fold, dx_recv, dx_part, dx_own,
    rbuf, gl, gl_c, gl_s, gl_y, gl_z,
    lsem_x, lsem_b, lsem_w, lsem_do, ssem, rsem,
):
    x = lax.axis_index("tp")
    z = lax.axis_index("sp_0")
    y = lax.axis_index("sp_1")
    c = lax.axis_index("sp_2")
    spi = (z * 4 + y) * 2 + c
    right = {"tp": (x + 1) % 4}
    left = {"tp": (x + 3) % 4}
    nxt = (spi + 1) % 32
    prv = (spi + 31) % 32
    sp_next = {"sp_0": nxt // 8, "sp_1": (nxt // 2) % 4, "sp_2": nxt % 2}
    sp_prev = {"sp_0": prv // 8, "sp_1": (prv // 2) % 4, "sp_2": prv % 2}
    partner = {"sp_2": 1 - c}
    ydev = [None] + [{"sp_1": (y + r) % 4} for r in (1, 2, 3)]
    zdev = [None] + [{"sp_0": (z + r) % 4} for r in (1, 2, 3)]
    yid = [(y + r) % 4 for r in range(4)]
    zid = [(z + r) % 4 for r in range(4)]
    src = [x, (x + 3) % 4, (x + 1) % 4, (x + 2) % 4]

    counter = [0]
    started = []

    def send(src_ref, dst_ref, dev):
        i = counter[0]
        counter[0] += 1
        cp = pltpu.make_async_remote_copy(
            src_ref=src_ref, dst_ref=dst_ref, send_sem=ssem.at[i], recv_sem=rsem.at[i],
            device_id=dev, device_id_type=MESH,
        )
        cp.start()
        started.append(cp)
        return cp

    x_copy = pltpu.make_async_copy(x_hbm, xbuf.at[:, pl.ds(0, 768)], lsem_x)
    x_copy.start()
    barrier = pltpu.get_barrier_semaphore()
    peers = [left, right, partner, sp_next, sp_prev] + ydev[1:] + zdev[1:]
    for dev in peers:
        pl.semaphore_signal(barrier, inc=1, device_id=dev, device_id_type=MESH)
    b_copy = pltpu.make_async_copy(rb_hbm, rbuf, lsem_b)
    gl[...] = jnp.zeros_like(gl)
    b_copy.start()
    x_copy.wait()
    pl.semaphore_wait(barrier, len(peers))

    order = (3, 2, 1, 0)
    from_left, from_right, opp_a, opp_b = {}, {}, {}, {}
    slot = [pl.ds(768 * i, 768) for i in range(4)]

    def send_own(j):
        rows = pl.ds(128 * j, 128)
        from_left[j] = send(xbuf.at[rows, slot[0]], xbuf.at[rows, slot[1]], right)
        from_right[j] = send(xbuf.at[rows, slot[0]], xbuf.at[rows, slot[2]], left)

    def forward(j):
        first, second = pl.ds(128 * j, 64), pl.ds(128 * j + 64, 64)
        from_left[j].wait_recv()
        opp_a[j] = send(xbuf.at[first, slot[1]], xbuf.at[first, slot[3]], right)
        from_right[j].wait_recv()
        opp_b[j] = send(xbuf.at[second, slot[2]], xbuf.at[second, slot[3]], left)

    def project_a(j):
        rows = pl.ds(128 * j, 128)

        def body(hp, carry):
            cols = pl.ds(pl.multiple_of(hp * 384, 128), 384)
            acc[j % 2, hp] = dot(xbuf[rows, 0:2304], w[0:2304, cols])
            return carry

        lax.fori_loop(0, 3, body, 0)

    def project_b(j):
        opp_a[j].wait_recv()
        opp_b[j].wait_recv()
        rows = pl.ds(128 * j, 128)
        ext = pl.ds(256 + 128 * j, 128)

        def body(hp, carry):
            cols = pl.ds(pl.multiple_of(hp * 384, 128), 384)
            out = (acc[j % 2, hp] + dot(xbuf[rows, 2304:3072], w[2304:3072, cols])).astype(BF)
            qs[hp, rows] = out[:, :128] * jnp.asarray(0.125, BF)
            kext[hp, ext] = out[:, 128:256]
            kt[hp, :, ext] = out[:, 128:256].T
            vext[hp, ext] = out[:, 256:]
            return carry

        lax.fori_loop(0, 3, body, 0)

    def transpose_rows(j):
        rows = pl.ds(128 * j, 128)
        for s in range(4):
            xt[src[s], :, rows] = xbuf[rows, slot[s]].T

    send_own(order[0])
    send_own(order[1])

    w_copies = []
    for s in range(4):
        for hp in range(3):
            for m, ref in enumerate((wq_hbm, wk_hbm, wv_hbm)):
                cp = pltpu.make_async_copy(
                    ref.at[pl.ds(src[s] * 768, 768), pl.ds(128 * hp, 128)],
                    w.at[slot[s], pl.ds(384 * hp + 128 * m, 128)],
                    lsem_w.at[(hp * 4 + s) * 3 + m],
                )
                cp.start()
                w_copies.append(cp)
    do_copies = []
    for hp in range(3):
        cp = pltpu.make_async_copy(do_hbm.at[:, pl.ds(128 * hp, 128)], do.at[hp], lsem_do.at[hp])
        cp.start()
        do_copies.append(cp)

    b_copy.wait()
    gl[0:6, 0:320] = rbuf[...]
    line = pltpu.roll(gl[...], 193, 1)
    lane = lax.broadcasted_iota(jnp.int32, (8, 512), 1)
    line = jnp.where((lane > 0) & (lane < 128), line[:, 0:1], line)
    gl[...] = line
    key_seg = lax.broadcasted_iota(jnp.int32, (384, 128), 0) // 64
    query_seg = lax.broadcasted_iota(jnp.int32, (384, 128), 1) // 64
    seen = (key_seg >= query_seg) & (key_seg <= query_seg + 4)
    for h in range(6):
        wide = jnp.broadcast_to(gl[h : h + 1, :], (384, 512))
        wide = pltpu.roll(wide, 0, 1, stride=1, stride_axis=0)
        bias[h // 2, :, pl.ds(128 * (h % 2), 128)] = jnp.where(seen, wide[:, :128], -jnp.inf)
    gbias[...] = jnp.zeros_like(gbias)
    dk_acc[...] = jnp.zeros_like(dk_acc)
    dv_acc[...] = jnp.zeros_like(dv_acc)

    for cp in w_copies + do_copies:
        cp.wait()

    forward(order[0])
    send_own(order[2])
    project_a(order[0])
    forward(order[1])
    send_own(order[3])
    project_a(order[1])
    project_b(order[0])
    transpose_rows(order[0])
    forward(order[2])
    project_a(order[2])
    project_b(order[1])
    halo_k = send(kext.at[:, pl.ds(512, 256)], kext.at[:, pl.ds(0, 256)], sp_next)
    halo_v = send(vext.at[:, pl.ds(512, 256)], vext.at[:, pl.ds(0, 256)], sp_next)
    transpose_rows(order[1])
    forward(order[3])
    project_a(order[3])
    project_b(order[2])

    lane_q = lax.broadcasted_iota(jnp.int32, (128, 128), 1)
    row_f = lax.broadcasted_iota(jnp.int32, (128, 128), 0)
    zero = jnp.zeros((128, 128), BF)

    def stacked(block):
        return jnp.concatenate(
            [jnp.where(lane_q < 64, block, zero), jnp.where(lane_q >= 64, block, zero)], axis=0
        )

    pen = jnp.where(spi == 0, -jnp.inf, 0.0).astype(F32)

    def unit(hp, qp):
        rows = pl.ds(qp * 128, 128)
        keys = pl.ds(qp * 128, 384)
        qm = stacked(qs[hp, rows])
        dm = stacked(do[hp, rows])
        score = dot(kext[hp, keys], qm, NT) + bias[hp]
        if qp < 2:
            cut = 256 - 128 * qp
            score = jnp.concatenate([score[:cut] + pen, score[cut:]], axis=0)
        top = jnp.max(score, axis=0, keepdims=True)
        e = jnp.exp(score - top)
        inv = 1.0 / jnp.sum(e, axis=0, keepdims=True)
        prob = e * inv
        low = prob.astype(BF)
        gp = dot(vext[hp, keys], dm, NT)
        delta = jnp.sum(low.astype(F32) * gp, axis=0, keepdims=True)
        ds = prob * (gp - delta)
        gbias[hp] += ds
        dlow = ds.astype(BF)
        dk_acc[hp, keys] += dot(dlow, qm)
        dv_acc[hp, keys] += dot(low, dm)
        dqt = dot(kt[hp, :, keys], dlow)
        dqt = jnp.where(row_f < 64, dqt[:, :128], dqt[:, 128:]) * 0.125
        g[rows, pl.ds(384 * hp, 128)] = dqt.T.astype(BF)

    def last_units():
        for hp in range(3):
            unit(hp, 3)

    last_units()
    project_b(order[3])
    halo_k.wait_recv()
    halo_v.wait_recv()
    for hp in range(3):
        kt[hp, :, 0:256] = kext[hp, 0:256].T

    halo_back = {}

    def attention(hp):
        unit(hp, 0)
        unit(hp, 1)
        hb_send[hp, 0] = dk_acc[hp, 0:256].astype(BF)
        hb_send[hp, 1] = dv_acc[hp, 0:256].astype(BF)
        halo_back[hp] = send(hb_send.at[hp], hb_recv.at[hp], sp_prev)
        unit(hp, 2)
        g[0:256, pl.ds(384 * hp + 128, 128)] = dk_acc[hp, 256:512].astype(BF)
        g[0:256, pl.ds(384 * hp + 256, 128)] = dv_acc[hp, 256:512].astype(BF)

    def finish_grads(hp):
        halo_back[hp].wait_recv()
        g[256:512, pl.ds(384 * hp + 128, 128)] = (
            dk_acc[hp, 512:768] + hb_recv[hp, 0].astype(F32)
        ).astype(BF)
        g[256:512, pl.ds(384 * hp + 256, 128)] = (
            dv_acc[hp, 512:768] + hb_recv[hp, 1].astype(F32)
        ).astype(BF)

    core_copy = {}

    def weight_grad(hp):
        def body(i, carry):
            out = dot(xt[i], g[:, 384 * hp : 384 * hp + 384]).astype(BF)
            dwb[hp, pl.ds(4 * i, 4)] = out.reshape(4, 2, 96, 384)
            return carry

        lax.fori_loop(0, 4, body, 0)
        core_copy[hp] = send(dwb.at[hp, :, 1 - c], crecv.at[hp], partner)

    lo, hi = pl.ds(0, 2), pl.ds(2, 2)
    ra, rb = pl.ds(0, 48), pl.ds(48, 48)
    st2 = {}

    def rs_start(hp):
        core_copy[hp].wait_recv()

        def body(i, carry):
            zz, yy = i // 4, i % 4
            s1[hp, zz, yy] = (dwb[hp, i, c].astype(F32) + crecv[hp, i].astype(F32)).astype(BF)
            return carry

        lax.fori_loop(0, 16, body, 0)
        f = {}
        f["ra"] = send(s1.at[hp, lo, yid[2], ra], fold.at[hp, 0], ydev[1])
        f["la"] = send(s1.at[hp, hi, yid[2], ra], fold.at[hp, 1], ydev[3])
        f["rb"] = send(s1.at[hp, zid[2], lo, rb], fold.at[hp, 2], zdev[1])
        f["lb"] = send(s1.at[hp, zid[2], hi, rb], fold.at[hp, 3], zdev[3])
        f["ura"] = send(s1.at[hp, hi, yid[1], ra], recv2.at[hp, 0, hi], ydev[1])
        f["ula"] = send(s1.at[hp, lo, yid[3], ra], recv2.at[hp, 1, lo], ydev[3])
        f["urb"] = send(s1.at[hp, zid[1], hi, rb], recv2.at[hp, 2, hi], zdev[1])
        f["ulb"] = send(s1.at[hp, zid[3], lo, rb], recv2.at[hp, 3, lo], zdev[3])
        st2[hp] = f

    def rs_fold(hp):
        f = st2[hp]

        def add(k, index):
            for i in range(2):
                at = index(i)
                s1[at] = (s1[at].astype(F32) + fold[hp, k, i].astype(F32)).astype(BF)

        f["ra"].wait_recv()
        add(0, lambda i: (hp, i, yid[1], ra))
        f["fra"] = send(s1.at[hp, lo, yid[1], ra], recv2.at[hp, 0, lo], ydev[1])
        f["la"].wait_recv()
        add(1, lambda i: (hp, 2 + i, yid[3], ra))
        f["fla"] = send(s1.at[hp, hi, yid[3], ra], recv2.at[hp, 1, hi], ydev[3])
        f["rb"].wait_recv()
        add(2, lambda i: (hp, zid[1], i, rb))
        f["frb"] = send(s1.at[hp, zid[1], lo, rb], recv2.at[hp, 2, lo], zdev[1])
        f["lb"].wait_recv()
        add(3, lambda i: (hp, zid[3], 2 + i, rb))
        f["flb"] = send(s1.at[hp, zid[3], hi, rb], recv2.at[hp, 3, hi], zdev[3])

    st3 = {}

    def rs_second(hp):
        f = st2[hp]
        for k in ("ura", "ula", "urb", "ulb", "fra", "fla", "frb", "flb"):
            f[k].wait_recv()
        for i in range(4):
            s2[hp, 0, i] = (
                s1[hp, i, y, ra].astype(F32)
                + recv2[hp, 0, i].astype(F32)
                + recv2[hp, 1, i].astype(F32)
            ).astype(BF)
            s2[hp, 1, i] = (
                s1[hp, z, i, rb].astype(F32)
                + recv2[hp, 2, i].astype(F32)
                + recv2[hp, 3, i].astype(F32)
            ).astype(BF)
        st3[hp] = [send(s2.at[hp, 0, zid[r]], recv3.at[hp, 0, r - 1], zdev[r]) for r in (1, 3, 2)]
        st3[hp] += [send(s2.at[hp, 1, yid[r]], recv3.at[hp, 1, r - 1], ydev[r]) for r in (1, 3, 2)]

    def rs_finish(hp):
        for cp in st3[hp]:
            cp.wait_recv()
        cols = pl.ds(128 * hp, 128)
        for part, own in ((0, z), (1, y)):
            total = s2[hp, part, own].astype(F32)
            for r in range(3):
                total += recv3[hp, part, r].astype(F32)
            rows = pl.ds(48 * part, 48)
            for m in range(3):
                gw_ref[m, rows, cols] = total[:, 128 * m : 128 * m + 128]

    def dx_block(t, s):
        return dot(w[slot[s], :], g[256 * t : 256 * t + 256, :], NT)

    dxc = {}
    half_a, half_b = pl.ds(0, 384), pl.ds(384, 384)

    def dx_opposite(t):
        out = dx_block(t, 3).astype(BF)
        dx_send[t, 0] = out[:384]
        dx_send[t, 1] = out[384:]
        dxc[t, "fr"] = send(dx_send.at[t, 0], dx_fold.at[t, 0], right)
        dxc[t, "fl"] = send(dx_send.at[t, 1], dx_fold.at[t, 1], left)

    def dx_direct(t):
        out = dx_block(t, 2)
        dx_send[t, 2] = out[384:].astype(BF)
        dxc[t, "ur"] = send(dx_send.at[t, 2], dx_recv.at[t, 0, half_b], right)
        dx_part[t, 0] = out[:384]
        out = dx_block(t, 1)
        dx_send[t, 3] = out[:384].astype(BF)
        dxc[t, "ul"] = send(dx_send.at[t, 3], dx_recv.at[t, 1, half_a], left)
        dx_part[t, 1] = out[384:]

    def dx_folded(t):
        dxc[t, "fr"].wait_recv()
        dx_send[t, 4] = (dx_part[t, 0] + dx_fold[t, 0].astype(F32)).astype(BF)
        dxc[t, "gr"] = send(dx_send.at[t, 4], dx_recv.at[t, 0, half_a], right)
        dxc[t, "fl"].wait_recv()
        dx_send[t, 5] = (dx_part[t, 1] + dx_fold[t, 1].astype(F32)).astype(BF)
        dxc[t, "gl"] = send(dx_send.at[t, 5], dx_recv.at[t, 1, half_b], left)

    def dx_mine(t):
        dx_own[t] = dx_block(t, 0)

    def dx_finish(t):
        for half, names in ((1, ("ur", "gl")), (0, ("ul", "gr"))):
            for k in names:
                dxc[t, k].wait_recv()
            rows = pl.ds(384 * half, 384)
            total = (
                dx_own[t, rows] + dx_recv[t, 0, rows].astype(F32) + dx_recv[t, 1, rows].astype(F32)
            )
            gx_ref[pl.ds(256 * t, 256), rows] = total.T.astype(BF)

    def bias_line():
        for hp in range(3):
            for par in range(2):
                total = jnp.zeros((8, 512), F32)
                for a in range(48):
                    part = gbias[hp, pl.ds(8 * a, 8), pl.ds(128 * par, 128)]
                    part = jnp.concatenate([part, jnp.zeros((8, 384), F32)], axis=1)
                    total += pltpu.roll(part, (512 - 8 * a) % 512, 1)
                sub = lax.broadcasted_iota(jnp.int32, (8, 512), 0)
                for bit in range(3):
                    moved = pltpu.roll(total, 512 - (1 << bit), 1)
                    total = jnp.where((sub >> bit) % 2 == 1, moved, total)
                h = 2 * hp + par
                gl[h : h + 1, :] = jnp.sum(total, axis=0, keepdims=True)
        gl[6:8, :] = jnp.zeros((2, 512), F32)

    attention(0)
    attention(1)
    attention(2)
    dx_opposite(0)
    dx_direct(0)
    transpose_rows(order[2])
    transpose_rows(order[3])
    finish_grads(0)
    weight_grad(0)
    finish_grads(1)
    finish_grads(2)
    dx_opposite(1)
    dx_direct(1)
    rs_start(0)
    weight_grad(1)
    dx_folded(0)
    rs_fold(0)
    weight_grad(2)
    rs_start(1)
    bias_line()
    gbc = send(gl, gl_c, partner)
    rs_second(0)
    rs_fold(1)
    rs_start(2)
    dx_folded(1)
    gbc.wait_recv()
    gl_s[0] = gl[...] + gl_c[...]
    gby = [send(gl_s.at[0], gl_y.at[r - 1], ydev[r]) for r in (1, 2, 3)]
    dx_mine(0)
    rs_second(1)
    rs_fold(2)
    dx_mine(1)
    rs_finish(0)
    for cp in gby:
        cp.wait_recv()
    gl_s[1] = gl_s[0] + gl_y[0] + gl_y[1] + gl_y[2]
    gbz = [send(gl_s.at[1], gl_z.at[r - 1], zdev[r]) for r in (1, 2, 3)]
    rs_second(2)
    rs_finish(1)
    dx_finish(0)
    for cp in gbz:
        cp.wait_recv()
    total = gl_s[1] + gl_z[0] + gl_z[1] + gl_z[2]
    far = jnp.sum(jnp.where(lane < 128, total, 0.0), axis=1, keepdims=True)
    total = jnp.where(lane == 0, far, total)
    total = pltpu.roll(total, 512 - 193, 1)
    gb_ref[...] = total[0:6, 0:320]
    rs_finish(2)
    dx_finish(1)
    for cp in started:
        cp.wait_send()


def write_out(gx, gw, gb, gx_out, gwq_out, gwk_out, gwv_out, gb_out, sem):
    pairs = [(gx, gx_out), (gw.at[0], gwq_out), (gw.at[1], gwk_out), (gw.at[2], gwv_out), (gb, gb_out)]
    copies = [pltpu.make_async_copy(a, b, sem.at[i]) for i, (a, b) in enumerate(pairs)]
    for cp in copies:
        cp.start()
    for cp in copies:
        cp.wait()


def local(inputs, w_query, w_key, w_value, rel_bias, d_out):
    any_spec = pl.BlockSpec(memory_space=pl.ANY)
    vmem = pl.BlockSpec(memory_space=pltpu.VMEM)
    V = pltpu.VMEM
    gx, gw, gb = pl.pallas_call(
        kernel,
        out_shape=(V((512, 768), BF), V((3, 96, 384), F32), V((6, 320), F32)),
        in_specs=[any_spec] * 6,
        out_specs=(vmem, vmem, vmem),
        scratch_shapes=[
            V((512, 3072), BF),
            V((3072, 1152), BF),
            V((4, 768, 512), BF),
            V((2, 3, 128, 384), F32),
            V((3, 768, 128), BF),
            V((3, 768, 128), BF),
            V((3, 512, 128), BF),
            V((3, 512, 128), BF),
            V((3, 128, 768), BF),
            V((3, 768, 128), F32),
            V((3, 768, 128), F32),
            V((3, 384, 256), F32),
            V((3, 384, 256), F32),
            V((512, 1152), BF),
            V((3, 2, 256, 128), BF),
            V((3, 2, 256, 128), BF),
            V((3, 16, 2, 96, 384), BF),
            V((3, 16, 96, 384), BF),
            V((3, 4, 4, 96, 384), BF),
            V((3, 4, 2, 48, 384), BF),
            V((3, 4, 4, 48, 384), BF),
            V((3, 2, 4, 48, 384), BF),
            V((3, 2, 3, 48, 384), BF),
            V((2, 6, 384, 256), BF),
            V((2, 2, 384, 256), BF),
            V((2, 2, 768, 256), BF),
            V((2, 2, 384, 256), F32),
            V((2, 768, 256), F32),
            V((6, 320), F32),
            V((8, 512), F32),
            V((8, 512), F32),
            V((2, 8, 512), F32),
            V((3, 8, 512), F32),
            V((3, 8, 512), F32),
            pltpu.SemaphoreType.DMA,
            pltpu.SemaphoreType.DMA,
            pltpu.SemaphoreType.DMA((36,)),
            pltpu.SemaphoreType.DMA((3,)),
            pltpu.SemaphoreType.DMA((NSEM,)),
            pltpu.SemaphoreType.DMA((NSEM,)),
        ],
        compiler_params=pltpu.CompilerParams(
            collective_id=0, has_side_effects=True, vmem_limit_bytes=58 * 1024 * 1024
        ),
    )(inputs, w_query, w_key, w_value, rel_bias.T, d_out)
    gx, gwq, gwk, gwv, gb = pl.pallas_call(
        write_out,
        out_shape=(
            jax.ShapeDtypeStruct((512, 768), BF),
            jax.ShapeDtypeStruct((96, 384), F32),
            jax.ShapeDtypeStruct((96, 384), F32),
            jax.ShapeDtypeStruct((96, 384), F32),
            jax.ShapeDtypeStruct((6, 320), F32),
        ),
        in_specs=[vmem] * 3,
        out_specs=[any_spec] * 5,
        scratch_shapes=[pltpu.SemaphoreType.DMA((5,))],
        compiler_params=pltpu.CompilerParams(vmem_limit_bytes=4 * 1024 * 1024),
    )(gx, gw, gb)
    return gx, gwq, gwk, gwv, gb.T


def solution(mesh):
    torus = Mesh(mesh.devices.reshape(4, 4, 2, mesh.shape["tp"]), ("sp_0", "sp_1", "sp_2", "tp"))
    return jax.shard_map(
        local,
        mesh=torus,
        in_specs=(
            P(SP, "tp"),
            P(None, "tp"),
            P(None, "tp"),
            P(None, "tp"),
            P(None, "tp"),
            P(SP, "tp"),
        ),
        out_specs=(P(SP, "tp"), P(SP, "tp"), P(SP, "tp"), P(SP, "tp"), P(None, "tp")),
        check_vma=False,
    )
```

```python
import functools

import jax
import jax.numpy as jnp
from jax import lax
from jax.experimental import pallas as pl
from jax.experimental.pallas import tpu as pltpu
from jax.sharding import Mesh
from jax.sharding import PartitionSpec as P

SP = ("sp_0", "sp_1", "sp_2")
MESH = pl.DeviceIdType.MESH
BF = jnp.bfloat16
F32 = jnp.float32
SENDS, RECVS = 10, 36

NN = (((1,), (0,)), ((), ()))
NT = (((1,), (1,)), ((), ()))


def dot(a, b, dims=NN):
    return lax.dot_general(a, b, dims, preferred_element_type=F32)


def kernel(
    x_hbm, wq_hbm, wk_hbm, wv_hbm, rb_hbm, do_hbm,
    gx_ref, gw_ref, gb_ref,
    xbuf, w, xt, acc, kext, vext, qs, do, kt, dk_acc, dv_acc, bias, gbias, g,
    hb_send, hb_recv, dwb, crecv, s1,
    fold, recv2, s2, recv3,
    dx_send, dx_fold, dx_recv, dx_part, dx_own,
    rbuf, gl, gl_c, gl_s, gl_r,
    lsem_x, lsem_b, lsem_w, lsem_do, ssem, rsem,
):
    x = lax.axis_index("tp")
    z = lax.axis_index("sp_0")
    y = lax.axis_index("sp_1")
    c = lax.axis_index("sp_2")
    spi = (z * 4 + y) * 2 + c
    right = {"tp": (x + 1) % 4}
    left = {"tp": (x + 3) % 4}
    nxt = (spi + 1) % 32
    prv = (spi + 31) % 32
    sp_next = {"sp_0": nxt // 8, "sp_1": (nxt // 2) % 4, "sp_2": nxt % 2}
    sp_prev = {"sp_0": prv // 8, "sp_1": (prv // 2) % 4, "sp_2": prv % 2}
    partner = {"sp_2": 1 - c}
    ydev = [None] + [{"sp_1": (y + r) % 4} for r in (1, 2, 3)]
    zdev = [None] + [{"sp_0": (z + r) % 4} for r in (1, 2, 3)]
    yid = [(y + r) % 4 for r in range(4)]
    zid = [(z + r) % 4 for r in range(4)]
    src = [x, (x + 3) % 4, (x + 1) % 4, (x + 2) % 4]

    sends, recvs = {}, {}

    def send(src_ref, dst_ref, dev, out, back):
        pltpu.make_async_remote_copy(
            src_ref=src_ref, dst_ref=dst_ref,
            send_sem=ssem.at[sends.setdefault(out, len(sends))],
            recv_sem=rsem.at[recvs.setdefault(back, len(recvs))],
            device_id=dev, device_id_type=MESH,
        ).start()

    def arrived(back, ref):
        pltpu.make_async_copy(ref, ref, rsem.at[recvs[back]]).wait()

    def sent(out, ref):
        pltpu.make_async_copy(ref, ref, ssem.at[sends[out]]).wait()

    x_copy = pltpu.make_async_copy(x_hbm, xbuf.at[:, pl.ds(0, 768)], lsem_x)
    x_copy.start()
    barrier = pltpu.get_barrier_semaphore()
    peers = [left, right, partner, sp_next, sp_prev] + ydev[1:] + zdev[1:]
    for dev in peers:
        pl.semaphore_signal(barrier, inc=1, device_id=dev, device_id_type=MESH)
    b_copy = pltpu.make_async_copy(rb_hbm, rbuf, lsem_b)
    gl[...] = jnp.zeros_like(gl)
    b_copy.start()
    x_copy.wait()
    pl.semaphore_wait(barrier, len(peers))

    order = (3, 2, 1, 0)
    slot = [pl.ds(768 * i, 768) for i in range(4)]

    def send_own(j):
        rows = pl.ds(128 * j, 128)
        send(xbuf.at[rows, slot[0]], xbuf.at[rows, slot[1]], right, "x", ("xl", j))
        send(xbuf.at[rows, slot[0]], xbuf.at[rows, slot[2]], left, "x", ("xr", j))

    def forward(j):
        rows, first, second = pl.ds(128 * j, 128), pl.ds(128 * j, 64), pl.ds(128 * j + 64, 64)
        arrived(("xl", j), xbuf.at[rows, slot[1]])
        send(xbuf.at[first, slot[1]], xbuf.at[first, slot[3]], right, "x", ("xo", j))
        arrived(("xr", j), xbuf.at[rows, slot[2]])
        send(xbuf.at[second, slot[2]], xbuf.at[second, slot[3]], left, "x", ("xo", j))

    def project_a(j):
        rows = pl.ds(128 * j, 128)

        def body(m, carry):
            cols = pl.ds(pl.multiple_of(m * 384, 128), 384)
            acc[j % 2, m] = dot(xbuf[rows, 0:2304], w[0:2304, cols])
            return carry

        lax.fori_loop(0, 3, body, 0)

    def project_b(j):
        rows = pl.ds(128 * j, 128)
        ext = pl.ds(256 + 128 * j, 128)
        arrived(("xo", j), xbuf.at[rows, slot[3]])
        for m in range(3):
            out = acc[j % 2, m] + dot(xbuf[rows, 2304:3072], w[2304:3072, 384 * m : 384 * m + 384])
            out = out.astype(BF)
            for hp in range(3):
                one = out[:, 128 * hp : 128 * hp + 128]
                if m == 0:
                    qs[hp, rows] = one * jnp.asarray(0.125, BF)
                elif m == 1:
                    kext[hp, ext] = one
                    kt[hp, :, ext] = one.T
                else:
                    vext[hp, ext] = one

    def transpose_rows(j):
        rows = pl.ds(128 * j, 128)
        for s in range(4):
            xt[src[s], :, rows] = xbuf[rows, slot[s]].T

    send_own(order[0])
    send_own(order[1])

    for i in range(4):
        for m, ref in enumerate((wq_hbm, wk_hbm, wv_hbm)):
            pltpu.make_async_copy(
                ref.at[pl.ds(src[i] * 768, 768)], w.at[slot[i], pl.ds(384 * m, 384)], lsem_w
            ).start()
    do_copy = pltpu.make_async_copy(do_hbm, do, lsem_do)
    do_copy.start()

    b_copy.wait()
    gl[0:6, 0:320] = rbuf[...]
    line = pltpu.roll(gl[...], 193, 1)
    lane = lax.broadcasted_iota(jnp.int32, (8, 512), 1)
    line = jnp.where((lane > 0) & (lane < 128), line[:, 0:1], line)
    gl[...] = line
    key_seg = lax.broadcasted_iota(jnp.int32, (384, 128), 0) // 64
    query_seg = lax.broadcasted_iota(jnp.int32, (384, 128), 1) // 64
    seen = (key_seg >= query_seg) & (key_seg <= query_seg + 4)
    for h in range(6):
        wide = jnp.broadcast_to(gl[h : h + 1, :], (384, 512))
        wide = pltpu.roll(wide, 0, 1, stride=1, stride_axis=0)
        bias[h // 2, :, pl.ds(128 * (h % 2), 128)] = jnp.where(seen, wide[:, :128], -jnp.inf)
    gbias[...] = jnp.zeros_like(gbias)
    dk_acc[...] = jnp.zeros_like(dk_acc)
    dv_acc[...] = jnp.zeros_like(dv_acc)

    pltpu.make_async_copy(w, w, lsem_w).wait()
    do_copy.wait()

    forward(order[0])
    send_own(order[2])
    project_a(order[0])
    forward(order[1])
    send_own(order[3])
    project_a(order[1])
    project_b(order[0])
    transpose_rows(order[0])
    forward(order[2])
    project_a(order[2])
    project_b(order[1])
    send(kext.at[:, pl.ds(512, 256)], kext.at[:, pl.ds(0, 256)], sp_next, "h", "hk")
    send(vext.at[:, pl.ds(512, 256)], vext.at[:, pl.ds(0, 256)], sp_next, "h", "hv")
    transpose_rows(order[1])
    forward(order[3])
    project_a(order[3])
    project_b(order[2])

    lane_q = lax.broadcasted_iota(jnp.int32, (128, 128), 1)
    row_f = lax.broadcasted_iota(jnp.int32, (128, 128), 0)
    zero = jnp.zeros((128, 128), BF)

    def stacked(block):
        return jnp.concatenate(
            [jnp.where(lane_q < 64, block, zero), jnp.where(lane_q >= 64, block, zero)], axis=0
        )

    pen = jnp.where(spi == 0, -jnp.inf, 0.0).astype(F32)

    def unit(hp, qp):
        rows = pl.ds(qp * 128, 128)
        keys = pl.ds(qp * 128, 384)
        qm = stacked(qs[hp, rows])
        dm = stacked(do[rows, 128 * hp : 128 * hp + 128])
        score = dot(kext[hp, keys], qm, NT) + bias[hp]
        if qp < 2:
            cut = 256 - 128 * qp
            score = jnp.concatenate([score[:cut] + pen, score[cut:]], axis=0)
        top = jnp.max(score, axis=0, keepdims=True)
        e = jnp.exp(score - top)
        inv = 1.0 / jnp.sum(e, axis=0, keepdims=True)
        prob = e * inv
        low = prob.astype(BF)
        gp = dot(vext[hp, keys], dm, NT)
        delta = jnp.sum(prob * gp, axis=0, keepdims=True)
        ds = prob * (gp - delta)
        gbias[hp] += ds
        dlow = ds.astype(BF)
        dk_acc[hp, keys] += dot(dlow, qm)
        dv_acc[hp, keys] += dot(low, dm)
        dqt = dot(kt[hp, :, keys], dlow)
        dqt = jnp.where(row_f < 64, dqt[:, :128], dqt[:, 128:]) * 0.125
        g[rows, pl.ds(128 * hp, 128)] = dqt.T.astype(BF)

    def last_units():
        for hp in range(3):
            unit(hp, 3)

    last_units()
    project_b(order[3])
    arrived("hk", kext.at[:, pl.ds(0, 256)])
    arrived("hv", vext.at[:, pl.ds(0, 256)])
    for hp in range(3):
        kt[hp, :, 0:256] = kext[hp, 0:256].T

    def attention():
        for hp in range(3):
            unit(hp, 0)
            unit(hp, 1)
        for hp in range(3):
            hb_send[hp, 0] = dk_acc[hp, 0:256].astype(BF)
            hb_send[hp, 1] = dv_acc[hp, 0:256].astype(BF)
        for hp in range(3):
            send(hb_send.at[hp], hb_recv.at[hp], sp_prev, "hb", ("hb", hp))
        for hp in range(3):
            unit(hp, 2)
        for hp in range(3):
            g[0:256, pl.ds(384 + 128 * hp, 128)] = dk_acc[hp, 256:512].astype(BF)
            g[0:256, pl.ds(768 + 128 * hp, 128)] = dv_acc[hp, 256:512].astype(BF)

    def finish_grads(hp):
        arrived(("hb", hp), hb_recv.at[hp])
        g[256:512, pl.ds(384 + 128 * hp, 128)] = (
            dk_acc[hp, 512:768] + hb_recv[hp, 0].astype(F32)
        ).astype(BF)
        g[256:512, pl.ds(768 + 128 * hp, 128)] = (
            dv_acc[hp, 512:768] + hb_recv[hp, 1].astype(F32)
        ).astype(BF)

    def weight_grad(hp):
        def body(i, carry):
            grads = jnp.concatenate(
                [g[:, 384 * m + 128 * hp : 384 * m + 128 * hp + 128] for m in range(3)], axis=1
            )
            out = dot(xt[i], grads).astype(BF)
            dwb[hp, pl.ds(4 * i, 4)] = out.reshape(4, 2, 96, 384)
            return carry

        lax.fori_loop(0, 4, body, 0)
        send(dwb.at[hp, :, 1 - c], crecv.at[hp], partner, "c", ("c", hp))

    lo, hi = pl.ds(0, 2), pl.ds(2, 2)
    ra, rb = pl.ds(0, 48), pl.ds(48, 48)

    def rs_start(hp):
        arrived(("c", hp), crecv.at[hp])

        def body(i, carry):
            zz, yy = i // 4, i % 4
            s1[hp, zz, yy] = (dwb[hp, i, c].astype(F32) + crecv[hp, i].astype(F32)).astype(BF)
            return carry

        lax.fori_loop(0, 16, body, 0)
        f, u = ("f", hp), ("u", hp)
        send(s1.at[hp, lo, yid[2], ra], fold.at[hp, 0], ydev[1], "f", f)
        send(s1.at[hp, hi, yid[2], ra], fold.at[hp, 1], ydev[3], "f", f)
        send(s1.at[hp, zid[2], lo, rb], fold.at[hp, 2], zdev[1], "f", f)
        send(s1.at[hp, zid[2], hi, rb], fold.at[hp, 3], zdev[3], "f", f)
        send(s1.at[hp, hi, yid[1], ra], recv2.at[hp, 0, hi], ydev[1], "u", u)
        send(s1.at[hp, lo, yid[3], ra], recv2.at[hp, 1, lo], ydev[3], "u", u)
        send(s1.at[hp, zid[1], hi, rb], recv2.at[hp, 2, hi], zdev[1], "u", u)
        send(s1.at[hp, zid[3], lo, rb], recv2.at[hp, 3, lo], zdev[3], "u", u)

    def rs_fold(hp):
        def add(k, index):
            for i in range(2):
                at = index(i)
                s1[at] = (s1[at].astype(F32) + fold[hp, k, i].astype(F32)).astype(BF)

        u = ("u", hp)
        arrived(("f", hp), fold.at[hp])
        add(0, lambda i: (hp, i, yid[1], ra))
        add(1, lambda i: (hp, 2 + i, yid[3], ra))
        add(2, lambda i: (hp, zid[1], i, rb))
        add(3, lambda i: (hp, zid[3], 2 + i, rb))
        send(s1.at[hp, lo, yid[1], ra], recv2.at[hp, 0, lo], ydev[1], "u", u)
        send(s1.at[hp, hi, yid[3], ra], recv2.at[hp, 1, hi], ydev[3], "u", u)
        send(s1.at[hp, zid[1], lo, rb], recv2.at[hp, 2, lo], zdev[1], "u", u)
        send(s1.at[hp, zid[3], hi, rb], recv2.at[hp, 3, hi], zdev[3], "u", u)

    def rs_second(hp):
        arrived(("u", hp), recv2.at[hp])
        for i in range(4):
            s2[hp, 0, i] = (
                s1[hp, i, y, ra].astype(F32)
                + recv2[hp, 0, i].astype(F32)
                + recv2[hp, 1, i].astype(F32)
            ).astype(BF)
            s2[hp, 1, i] = (
                s1[hp, z, i, rb].astype(F32)
                + recv2[hp, 2, i].astype(F32)
                + recv2[hp, 3, i].astype(F32)
            ).astype(BF)
        for r in (1, 3, 2):
            send(s2.at[hp, 0, zid[r]], recv3.at[hp, 0, r - 1], zdev[r], "t", ("t", hp))
            send(s2.at[hp, 1, yid[r]], recv3.at[hp, 1, r - 1], ydev[r], "t", ("t", hp))

    def rs_finish(hp):
        arrived(("t", hp), recv3.at[hp])
        cols = pl.ds(128 * hp, 128)
        for part, own in ((0, z), (1, y)):
            total = s2[hp, part, own].astype(F32)
            for r in range(3):
                total += recv3[hp, part, r].astype(F32)
            rows = pl.ds(48 * part, 48)
            for m in range(3):
                gw_ref[m, rows, cols] = total[:, 128 * m : 128 * m + 128]

    def dx_block(t, s):
        return dot(w[slot[s], :], g[256 * t : 256 * t + 256, :], NT)

    half_a, half_b = pl.ds(0, 384), pl.ds(384, 384)

    def dx_opposite(t):
        out = dx_block(t, 3).astype(BF)
        dx_send[t, 0] = out[:384]
        dx_send[t, 1] = out[384:]
        send(dx_send.at[t, 0], dx_fold.at[t, 0], right, "d", ("df", t))
        send(dx_send.at[t, 1], dx_fold.at[t, 1], left, "d", ("df", t))

    def dx_direct(t):
        out = dx_block(t, 2).astype(BF)
        dx_send[t, 2] = out[384:]
        send(dx_send.at[t, 2], dx_recv.at[t, 0, half_b], right, "d", ("d", t))
        dx_part[t, 0] = out[:384]
        out = dx_block(t, 1).astype(BF)
        dx_send[t, 3] = out[:384]
        send(dx_send.at[t, 3], dx_recv.at[t, 1, half_a], left, "d", ("d", t))
        dx_part[t, 1] = out[384:]

    def dx_folded(t):
        arrived(("df", t), dx_fold.at[t])
        dx_send[t, 4] = (dx_part[t, 0].astype(F32) + dx_fold[t, 0].astype(F32)).astype(BF)
        send(dx_send.at[t, 4], dx_recv.at[t, 0, half_a], right, "d", ("d", t))
        dx_send[t, 5] = (dx_part[t, 1].astype(F32) + dx_fold[t, 1].astype(F32)).astype(BF)
        send(dx_send.at[t, 5], dx_recv.at[t, 1, half_b], left, "d", ("d", t))

    def dx_mine(t):
        dx_own[t] = dx_block(t, 0).astype(BF)

    def dx_finish(t):
        arrived(("d", t), dx_recv.at[t])
        total = (
            dx_own[t].astype(F32) + dx_recv[t, 0].astype(F32) + dx_recv[t, 1].astype(F32)
        )
        gx_ref[pl.ds(256 * t, 256), :] = total.T.astype(BF)

    def bias_line():
        for hp in range(3):
            for par in range(2):
                total = jnp.zeros((8, 512), F32)
                for a in range(48):
                    part = gbias[hp, pl.ds(8 * a, 8), pl.ds(128 * par, 128)]
                    part = jnp.concatenate([part, jnp.zeros((8, 384), F32)], axis=1)
                    total += pltpu.roll(part, (512 - 8 * a) % 512, 1)
                sub = lax.broadcasted_iota(jnp.int32, (8, 512), 0)
                for bit in range(3):
                    moved = pltpu.roll(total, 512 - (1 << bit), 1)
                    total = jnp.where((sub >> bit) % 2 == 1, moved, total)
                h = 2 * hp + par
                gl[h : h + 1, :] = jnp.sum(total, axis=0, keepdims=True)
        gl[6:8, :] = jnp.zeros((2, 512), F32)

    attention()
    dx_opposite(0)
    dx_direct(0)
    transpose_rows(order[2])
    transpose_rows(order[3])
    finish_grads(0)
    weight_grad(0)
    finish_grads(1)
    weight_grad(1)
    dx_folded(0)
    rs_start(0)
    finish_grads(2)
    weight_grad(2)
    dx_opposite(1)
    rs_fold(0)
    rs_start(1)
    dx_direct(1)
    rs_start(2)
    rs_fold(1)
    dx_mine(0)
    bias_line()
    send(gl, gl_c, partner, "gc", "gc")
    rs_second(0)
    dx_mine(1)
    rs_fold(2)
    arrived("gc", gl_c)
    gl_s[0] = gl[...] + gl_c[...]
    for r in (1, 2, 3):
        send(gl_s.at[0], gl_r.at[r - 1], ydev[r], "gr", "gy")
    dx_folded(1)
    rs_second(1)
    arrived("gy", gl_r.at[pl.ds(0, 3)])
    gl_s[1] = gl_s[0] + gl_r[0] + gl_r[1] + gl_r[2]
    for r in (1, 2, 3):
        send(gl_s.at[1], gl_r.at[2 + r], zdev[r], "gr", "gz")
    rs_finish(0)
    dx_finish(0)
    rs_second(2)
    rs_finish(1)
    arrived("gz", gl_r.at[pl.ds(3, 3)])
    total = gl_s[1] + gl_r[3] + gl_r[4] + gl_r[5]
    far = jnp.sum(jnp.where(lane < 128, total, 0.0), axis=1, keepdims=True)
    total = jnp.where(lane == 0, far, total)
    total = pltpu.roll(total, 512 - 193, 1)
    gb_ref[...] = total[0:6, 0:320]
    rs_finish(2)
    dx_finish(1)
    sent("x", xbuf.at[:, pl.ds(0, 2304)])
    sent("h", kext.at[:, pl.ds(0, 512)])
    sent("hb", hb_send)
    sent("c", crecv)
    sent("f", fold)
    sent("u", recv2)
    sent("t", recv3)
    sent("d", dx_send)
    sent("gc", gl_c)
    sent("gr", gl_r)
    assert len(sends) == SENDS and len(recvs) == RECVS, (len(sends), len(recvs))


def write_out(gx, gw, gb, gx_out, gwq_out, gwk_out, gwv_out, gb_out, sem):
    pairs = [(gx, gx_out), (gw.at[0], gwq_out), (gw.at[1], gwk_out), (gw.at[2], gwv_out), (gb, gb_out)]
    copies = [pltpu.make_async_copy(a, b, sem.at[i]) for i, (a, b) in enumerate(pairs)]
    for cp in copies:
        cp.start()
    for cp in copies:
        cp.wait()


def local(inputs, w_query, w_key, w_value, rel_bias, d_out):
    any_spec = pl.BlockSpec(memory_space=pl.ANY)
    vmem = pl.BlockSpec(memory_space=pltpu.VMEM)
    V = pltpu.VMEM
    gx, gw, gb = pl.pallas_call(
        kernel,
        out_shape=(V((512, 768), BF), V((3, 96, 384), F32), V((6, 320), F32)),
        in_specs=[any_spec] * 6,
        out_specs=(vmem, vmem, vmem),
        scratch_shapes=[
            V((512, 3072), BF),
            V((3072, 1152), BF),
            V((4, 768, 512), BF),
            V((2, 3, 128, 384), F32),
            V((3, 768, 128), BF),
            V((3, 768, 128), BF),
            V((3, 512, 128), BF),
            V((512, 384), BF),
            V((3, 128, 768), BF),
            V((3, 768, 128), F32),
            V((3, 768, 128), F32),
            V((3, 384, 256), F32),
            V((3, 384, 256), F32),
            V((512, 1152), BF),
            V((3, 2, 256, 128), BF),
            V((3, 2, 256, 128), BF),
            V((3, 16, 2, 96, 384), BF),
            V((3, 16, 96, 384), BF),
            V((3, 4, 4, 96, 384), BF),
            V((3, 4, 2, 48, 384), BF),
            V((3, 4, 4, 48, 384), BF),
            V((3, 2, 4, 48, 384), BF),
            V((3, 2, 3, 48, 384), BF),
            V((2, 6, 384, 256), BF),
            V((2, 2, 384, 256), BF),
            V((2, 2, 768, 256), BF),
            V((2, 2, 384, 256), BF),
            V((2, 768, 256), BF),
            V((6, 320), F32),
            V((8, 512), F32),
            V((8, 512), F32),
            V((2, 8, 512), F32),
            V((6, 8, 512), F32),
            pltpu.SemaphoreType.DMA,
            pltpu.SemaphoreType.DMA,
            pltpu.SemaphoreType.DMA,
            pltpu.SemaphoreType.DMA,
            pltpu.SemaphoreType.DMA((SENDS,)),
            pltpu.SemaphoreType.DMA((RECVS,)),
        ],
        compiler_params=pltpu.CompilerParams(
            collective_id=0, has_side_effects=True, vmem_limit_bytes=58 * 1024 * 1024
        ),
    )(inputs, w_query, w_key, w_value, rel_bias.T, d_out)
    gx, gwq, gwk, gwv, gb = pl.pallas_call(
        write_out,
        out_shape=(
            jax.ShapeDtypeStruct((512, 768), BF),
            jax.ShapeDtypeStruct((96, 384), F32),
            jax.ShapeDtypeStruct((96, 384), F32),
            jax.ShapeDtypeStruct((96, 384), F32),
            jax.ShapeDtypeStruct((6, 320), F32),
        ),
        in_specs=[vmem] * 3,
        out_specs=[any_spec] * 5,
        scratch_shapes=[pltpu.SemaphoreType.DMA((5,))],
        compiler_params=pltpu.CompilerParams(vmem_limit_bytes=4 * 1024 * 1024),
    )(gx, gw, gb)
    return gx, gwq, gwk, gwv, gb.T


def solution(mesh):
    torus = Mesh(mesh.devices.reshape(4, 4, 2, mesh.shape["tp"]), ("sp_0", "sp_1", "sp_2", "tp"))
    return jax.shard_map(
        local,
        mesh=torus,
        in_specs=(
            P(SP, "tp"),
            P(None, "tp"),
            P(None, "tp"),
            P(None, "tp"),
            P(None, "tp"),
            P(SP, "tp"),
        ),
        out_specs=(P(SP, "tp"), P(SP, "tp"), P(SP, "tp"), P(SP, "tp"), P(None, "tp")),
        check_vma=False,
    )
```

```python
import functools

import jax
import jax.numpy as jnp
from jax import lax
from jax.experimental import pallas as pl
from jax.experimental.pallas import tpu as pltpu
from jax.sharding import Mesh
from jax.sharding import PartitionSpec as P

SP = ("sp_0", "sp_1", "sp_2")
MESH = pl.DeviceIdType.MESH
BF = jnp.bfloat16
F32 = jnp.float32
SENDS, RECVS = 10, 36

NN = (((1,), (0,)), ((), ()))
NT = (((1,), (1,)), ((), ()))


def dot(a, b, dims=NN):
    return lax.dot_general(a, b, dims, preferred_element_type=F32)


def kernel(
    x_hbm, wq_hbm, wk_hbm, wv_hbm, rb_hbm, do_hbm,
    gx_ref, gw_ref, gb_ref,
    xbuf, w, xt, acc, kext, vext, qs, do, kt, dk_acc, dv_acc, bias, gbias, g,
    hb_send, hb_recv, dwb, crecv, s1,
    fold, recv2, s2, recv3,
    dx_send, dx_fold, dx_recv, dx_part, dx_own,
    rbuf, gl, gl_c, gl_s, gl_r,
    lsem_x, lsem_b, lsem_w, lsem_do, ssem, rsem,
):
    x = lax.axis_index("tp")
    z = lax.axis_index("sp_0")
    y = lax.axis_index("sp_1")
    c = lax.axis_index("sp_2")
    spi = (z * 4 + y) * 2 + c
    right = {"tp": (x + 1) % 4}
    left = {"tp": (x + 3) % 4}
    nxt = (spi + 1) % 32
    prv = (spi + 31) % 32
    sp_next = {"sp_0": nxt // 8, "sp_1": (nxt // 2) % 4, "sp_2": nxt % 2}
    sp_prev = {"sp_0": prv // 8, "sp_1": (prv // 2) % 4, "sp_2": prv % 2}
    partner = {"sp_2": 1 - c}
    ydev = [None] + [{"sp_1": (y + r) % 4} for r in (1, 2, 3)]
    zdev = [None] + [{"sp_0": (z + r) % 4} for r in (1, 2, 3)]
    yid = [(y + r) % 4 for r in range(4)]
    zid = [(z + r) % 4 for r in range(4)]
    src = [x, (x + 3) % 4, (x + 1) % 4, (x + 2) % 4]

    sends, recvs = {}, {}

    def send(src_ref, dst_ref, dev, out, back):
        pltpu.make_async_remote_copy(
            src_ref=src_ref, dst_ref=dst_ref,
            send_sem=ssem.at[sends.setdefault(out, len(sends))],
            recv_sem=rsem.at[recvs.setdefault(back, len(recvs))],
            device_id=dev, device_id_type=MESH,
        ).start()

    def arrived(back, ref):
        pltpu.make_async_copy(ref, ref, rsem.at[recvs[back]]).wait()

    def sent(out, ref):
        pltpu.make_async_copy(ref, ref, ssem.at[sends[out]]).wait()

    x_copy = pltpu.make_async_copy(x_hbm, xbuf.at[:, pl.ds(0, 768)], lsem_x)
    x_copy.start()
    barrier = pltpu.get_barrier_semaphore()
    peers = [left, right, partner, sp_next, sp_prev] + ydev[1:] + zdev[1:]
    for dev in peers:
        pl.semaphore_signal(barrier, inc=1, device_id=dev, device_id_type=MESH)
    b_copy = pltpu.make_async_copy(rb_hbm, rbuf, lsem_b)
    gl[...] = jnp.zeros_like(gl)
    b_copy.start()
    x_copy.wait()
    pl.semaphore_wait(barrier, len(peers))

    order = (3, 2, 1, 0)
    slot = [pl.ds(768 * i, 768) for i in range(4)]

    def send_own(j):
        rows = pl.ds(128 * j, 128)
        send(xbuf.at[rows, slot[0]], xbuf.at[rows, slot[1]], right, "x", ("xl", j))
        send(xbuf.at[rows, slot[0]], xbuf.at[rows, slot[2]], left, "x", ("xr", j))

    def forward(j):
        rows, first, second = pl.ds(128 * j, 128), pl.ds(128 * j, 64), pl.ds(128 * j + 64, 64)
        arrived(("xl", j), xbuf.at[rows, slot[1]])
        send(xbuf.at[first, slot[1]], xbuf.at[first, slot[3]], right, "x", ("xo", j))
        arrived(("xr", j), xbuf.at[rows, slot[2]])
        send(xbuf.at[second, slot[2]], xbuf.at[second, slot[3]], left, "x", ("xo", j))

    def project_a(j):
        rows = pl.ds(128 * j, 128)

        def body(m, carry):
            cols = pl.ds(pl.multiple_of(m * 384, 128), 384)
            acc[j % 2, m] = dot(xbuf[rows, 0:2304], w[0:2304, cols])
            return carry

        lax.fori_loop(0, 3, body, 0)

    def project_b(j):
        rows = pl.ds(128 * j, 128)
        ext = pl.ds(256 + 128 * j, 128)
        arrived(("xo", j), xbuf.at[rows, slot[3]])
        for m in range(3):
            out = acc[j % 2, m] + dot(xbuf[rows, 2304:3072], w[2304:3072, 384 * m : 384 * m + 384])
            out = out.astype(BF)
            for hp in range(3):
                one = out[:, 128 * hp : 128 * hp + 128]
                if m == 0:
                    qs[hp, rows] = one * jnp.asarray(0.125, BF)
                elif m == 1:
                    kext[hp, ext] = one
                    kt[hp, :, ext] = one.T
                else:
                    vext[hp, ext] = one

    def transpose_rows(j, slots=(0, 1, 2, 3)):
        rows = pl.ds(128 * j, 128)
        for s in slots:
            xt[src[s], :, rows] = xbuf[rows, slot[s]].T

    send_own(order[0])
    send_own(order[1])

    for i in range(4):
        for m, ref in enumerate((wq_hbm, wk_hbm, wv_hbm)):
            pltpu.make_async_copy(
                ref.at[pl.ds(src[i] * 768, 768)], w.at[slot[i], pl.ds(384 * m, 384)], lsem_w
            ).start()
    do_copy = pltpu.make_async_copy(do_hbm, do, lsem_do)
    do_copy.start()

    b_copy.wait()
    gl[0:6, 0:320] = rbuf[...]
    line = pltpu.roll(gl[...], 193, 1)
    lane = lax.broadcasted_iota(jnp.int32, (8, 512), 1)
    line = jnp.where((lane > 0) & (lane < 128), line[:, 0:1], line)
    gl[...] = line
    key_seg = lax.broadcasted_iota(jnp.int32, (384, 128), 0) // 64
    query_seg = lax.broadcasted_iota(jnp.int32, (384, 128), 1) // 64
    seen = (key_seg >= query_seg) & (key_seg <= query_seg + 4)
    for h in range(6):
        wide = jnp.broadcast_to(gl[h : h + 1, :], (384, 512))
        wide = pltpu.roll(wide, 0, 1, stride=1, stride_axis=0)
        bias[h // 2, :, pl.ds(128 * (h % 2), 128)] = jnp.where(seen, wide[:, :128], -jnp.inf)
    gbias[...] = jnp.zeros_like(gbias)
    dk_acc[...] = jnp.zeros_like(dk_acc)
    dv_acc[...] = jnp.zeros_like(dv_acc)

    pltpu.make_async_copy(w, w, lsem_w).wait()
    do_copy.wait()

    forward(order[0])
    send_own(order[2])
    project_a(order[0])
    forward(order[1])
    send_own(order[3])
    project_a(order[1])
    project_b(order[0])
    transpose_rows(order[0])
    forward(order[2])
    project_a(order[2])
    project_b(order[1])
    send(kext.at[:, pl.ds(512, 256)], kext.at[:, pl.ds(0, 256)], sp_next, "h", "hk")
    send(vext.at[:, pl.ds(512, 256)], vext.at[:, pl.ds(0, 256)], sp_next, "h", "hv")
    transpose_rows(order[1])
    transpose_rows(order[2], (0, 1, 2))
    forward(order[3])
    project_a(order[3])
    project_b(order[2])

    lane_q = lax.broadcasted_iota(jnp.int32, (128, 128), 1)
    row_f = lax.broadcasted_iota(jnp.int32, (128, 128), 0)
    zero = jnp.zeros((128, 128), BF)

    def stacked(block):
        return jnp.concatenate(
            [jnp.where(lane_q < 64, block, zero), jnp.where(lane_q >= 64, block, zero)], axis=0
        )

    pen = jnp.where(spi == 0, -jnp.inf, 0.0).astype(F32)

    def unit(hp, qp):
        rows = pl.ds(qp * 128, 128)
        keys = pl.ds(qp * 128, 384)
        qm = stacked(qs[hp, rows])
        dm = stacked(do[rows, 128 * hp : 128 * hp + 128])
        score = dot(kext[hp, keys], qm, NT) + bias[hp]
        if qp < 2:
            cut = 256 - 128 * qp
            score = jnp.concatenate([score[:cut] + pen, score[cut:]], axis=0)
        top = jnp.max(score, axis=0, keepdims=True)
        e = jnp.exp(score - top)
        inv = 1.0 / jnp.sum(e, axis=0, keepdims=True)
        prob = e * inv
        low = prob.astype(BF)
        gp = dot(vext[hp, keys], dm, NT)
        delta = jnp.sum(prob * gp, axis=0, keepdims=True)
        ds = prob * (gp - delta)
        gbias[hp] += ds
        dlow = ds.astype(BF)
        dk_acc[hp, keys] += dot(dlow, qm)
        dv_acc[hp, keys] += dot(low, dm)
        dqt = dot(kt[hp, :, keys], dlow)
        dqt = jnp.where(row_f < 64, dqt[:, :128], dqt[:, 128:]) * 0.125
        g[rows, pl.ds(128 * hp, 128)] = dqt.T.astype(BF)

    def last_units():
        for hp in range(3):
            unit(hp, 3)

    last_units()
    project_b(order[3])
    arrived("hk", kext.at[:, pl.ds(0, 256)])
    arrived("hv", vext.at[:, pl.ds(0, 256)])
    for hp in range(3):
        kt[hp, :, 0:256] = kext[hp, 0:256].T

    def send_halo_grads(heads):
        for hp in heads:
            hb_send[hp, 0] = dk_acc[hp, 0:256].astype(BF)
            hb_send[hp, 1] = dv_acc[hp, 0:256].astype(BF)
        for hp in heads:
            send(hb_send.at[hp], hb_recv.at[hp], sp_prev, "hb", ("hb", hp))

    def attention_first():
        for hp in (0, 1):
            unit(hp, 0)
            unit(hp, 1)
        send_halo_grads((0, 1))

    def attention_rest():
        for hp, qp in ((2, 0), (2, 1), (0, 2), (1, 2), (2, 2)):
            unit(hp, qp)
        for hp in range(3):
            g[0:256, pl.ds(384 + 128 * hp, 128)] = dk_acc[hp, 256:512].astype(BF)
            g[0:256, pl.ds(768 + 128 * hp, 128)] = dv_acc[hp, 256:512].astype(BF)
        send_halo_grads((2,))

    def finish_grads(hp):
        arrived(("hb", hp), hb_recv.at[hp])
        g[256:512, pl.ds(384 + 128 * hp, 128)] = (
            dk_acc[hp, 512:768] + hb_recv[hp, 0].astype(F32)
        ).astype(BF)
        g[256:512, pl.ds(768 + 128 * hp, 128)] = (
            dv_acc[hp, 512:768] + hb_recv[hp, 1].astype(F32)
        ).astype(BF)

    def weight_grad(m):
        for i in range(4):
            out = dot(xt[i], g[:, 384 * m : 384 * m + 384]).astype(BF)
            part = pl.ds(4 * i, 4)
            dwb[m, part] = out.reshape(4, 2, 96, 384)
            send(dwb.at[m, part, 1 - c], crecv.at[m, part], partner, "c", ("c", m))

    lo, hi = pl.ds(0, 2), pl.ds(2, 2)
    ra, rb = pl.ds(0, 48), pl.ds(48, 48)

    def rs_start(m):
        arrived(("c", m), crecv.at[m])

        def body(i, carry):
            zz, yy = i // 4, i % 4
            s1[m, zz, yy] = (dwb[m, i, c].astype(F32) + crecv[m, i].astype(F32)).astype(BF)
            return carry

        lax.fori_loop(0, 16, body, 0)
        f, u = ("f", m), ("u", m)
        send(s1.at[m, lo, yid[2], ra], fold.at[m, 0], ydev[1], "f", f)
        send(s1.at[m, hi, yid[2], ra], fold.at[m, 1], ydev[3], "f", f)
        send(s1.at[m, zid[2], lo, rb], fold.at[m, 2], zdev[1], "f", f)
        send(s1.at[m, zid[2], hi, rb], fold.at[m, 3], zdev[3], "f", f)
        send(s1.at[m, hi, yid[1], ra], recv2.at[m, 0, hi], ydev[1], "u", u)
        send(s1.at[m, lo, yid[3], ra], recv2.at[m, 1, lo], ydev[3], "u", u)
        send(s1.at[m, zid[1], hi, rb], recv2.at[m, 2, hi], zdev[1], "u", u)
        send(s1.at[m, zid[3], lo, rb], recv2.at[m, 3, lo], zdev[3], "u", u)

    def rs_fold(m):
        def add(k, index):
            for i in range(2):
                at = index(i)
                s1[at] = (s1[at].astype(F32) + fold[m, k, i].astype(F32)).astype(BF)

        u = ("u", m)
        arrived(("f", m), fold.at[m])
        add(0, lambda i: (m, i, yid[1], ra))
        add(1, lambda i: (m, 2 + i, yid[3], ra))
        add(2, lambda i: (m, zid[1], i, rb))
        add(3, lambda i: (m, zid[3], 2 + i, rb))
        send(s1.at[m, lo, yid[1], ra], recv2.at[m, 0, lo], ydev[1], "u", u)
        send(s1.at[m, hi, yid[3], ra], recv2.at[m, 1, hi], ydev[3], "u", u)
        send(s1.at[m, zid[1], lo, rb], recv2.at[m, 2, lo], zdev[1], "u", u)
        send(s1.at[m, zid[3], hi, rb], recv2.at[m, 3, hi], zdev[3], "u", u)

    def rs_second(m):
        arrived(("u", m), recv2.at[m])
        for i in range(4):
            s2[m, 0, i] = (
                s1[m, i, y, ra].astype(F32)
                + recv2[m, 0, i].astype(F32)
                + recv2[m, 1, i].astype(F32)
            ).astype(BF)
            s2[m, 1, i] = (
                s1[m, z, i, rb].astype(F32)
                + recv2[m, 2, i].astype(F32)
                + recv2[m, 3, i].astype(F32)
            ).astype(BF)
        for r in (1, 3, 2):
            send(s2.at[m, 0, zid[r]], recv3.at[m, 0, r - 1], zdev[r], "t", ("t", m))
            send(s2.at[m, 1, yid[r]], recv3.at[m, 1, r - 1], ydev[r], "t", ("t", m))

    def rs_finish(m):
        arrived(("t", m), recv3.at[m])
        for part, own in ((0, z), (1, y)):
            total = s2[m, part, own].astype(F32)
            for r in range(3):
                total += recv3[m, part, r].astype(F32)
            gw_ref[m, pl.ds(48 * part, 48), :] = total

    def dx_block(t, s, start=0, size=768):
        rows = slice(768 * s + start, 768 * s + start + size)
        return dot(w[rows, :], g[256 * t : 256 * t + 256, :], NT).astype(BF)

    half_a, half_b = pl.ds(0, 384), pl.ds(384, 384)

    def dx_opposite(t):
        first, second = dx_block(t, 3, 0, 384), dx_block(t, 3, 384, 384)
        dx_send[t, 0] = first
        dx_send[t, 1] = second
        send(dx_send.at[t, 0], dx_fold.at[t, 0], right, "d", ("df", t))
        send(dx_send.at[t, 1], dx_fold.at[t, 1], left, "d", ("df", t))

    def dx_direct(t):
        for_right, for_left = dx_block(t, 2), dx_block(t, 1)
        dx_send[t, 2] = for_right[384:]
        dx_part[t, 0] = for_right[:384]
        dx_send[t, 3] = for_left[:384]
        dx_part[t, 1] = for_left[384:]
        send(dx_send.at[t, 2], dx_recv.at[t, 0, half_b], right, "d", ("d", t))
        send(dx_send.at[t, 3], dx_recv.at[t, 1, half_a], left, "d", ("d", t))

    def dx_folded(t):
        arrived(("df", t), dx_fold.at[t])
        dx_send[t, 4] = (dx_part[t, 0].astype(F32) + dx_fold[t, 0].astype(F32)).astype(BF)
        dx_send[t, 5] = (dx_part[t, 1].astype(F32) + dx_fold[t, 1].astype(F32)).astype(BF)
        send(dx_send.at[t, 4], dx_recv.at[t, 0, half_a], right, "d", ("d", t))
        send(dx_send.at[t, 5], dx_recv.at[t, 1, half_b], left, "d", ("d", t))

    def dx_mine():
        first, second = dx_block(0, 0), dx_block(1, 0)
        dx_own[0] = first
        dx_own[1] = second

    def dx_finish(t):
        arrived(("d", t), dx_recv.at[t])
        total = (
            dx_own[t].astype(F32) + dx_recv[t, 0].astype(F32) + dx_recv[t, 1].astype(F32)
        )
        gx_ref[pl.ds(256 * t, 256), :] = total.T.astype(BF)

    def bias_line():
        for hp in range(3):
            for par in range(2):
                total = jnp.zeros((8, 512), F32)
                for a in range(48):
                    part = gbias[hp, pl.ds(8 * a, 8), pl.ds(128 * par, 128)]
                    part = jnp.concatenate([part, jnp.zeros((8, 384), F32)], axis=1)
                    total += pltpu.roll(part, (512 - 8 * a) % 512, 1)
                sub = lax.broadcasted_iota(jnp.int32, (8, 512), 0)
                for bit in range(3):
                    moved = pltpu.roll(total, 512 - (1 << bit), 1)
                    total = jnp.where((sub >> bit) % 2 == 1, moved, total)
                h = 2 * hp + par
                gl[h : h + 1, :] = jnp.sum(total, axis=0, keepdims=True)
        gl[6:8, :] = jnp.zeros((2, 512), F32)

    attention_first()
    attention_rest()
    dx_opposite(0)
    dx_direct(0)
    transpose_rows(order[2], (3,))
    transpose_rows(order[3])
    weight_grad(0)
    bias_line()
    send(gl, gl_c, partner, "gc", "gc")
    finish_grads(0)
    finish_grads(1)
    finish_grads(2)
    dx_opposite(1)
    arrived("gc", gl_c)
    gl_s[0] = gl[...] + gl_c[...]
    for r in (1, 2, 3):
        send(gl_s.at[0], gl_r.at[r - 1], ydev[r], "gr", "gy")
    rs_start(0)
    weight_grad(1)
    dx_folded(0)
    dx_direct(1)
    arrived("gy", gl_r.at[pl.ds(0, 3)])
    gl_s[1] = gl_s[0] + gl_r[0] + gl_r[1] + gl_r[2]
    for r in (1, 2, 3):
        send(gl_s.at[1], gl_r.at[2 + r], zdev[r], "gr", "gz")
    rs_start(1)
    rs_fold(0)
    weight_grad(2)
    rs_start(2)
    rs_fold(1)
    dx_mine()
    dx_folded(1)
    rs_second(0)
    rs_fold(2)
    rs_second(1)
    dx_finish(0)
    rs_finish(0)
    rs_second(2)
    rs_finish(1)
    dx_finish(1)
    arrived("gz", gl_r.at[pl.ds(3, 3)])
    total = gl_s[1] + gl_r[3] + gl_r[4] + gl_r[5]
    far = jnp.sum(jnp.where(lane < 128, total, 0.0), axis=1, keepdims=True)
    total = jnp.where(lane == 0, far, total)
    total = pltpu.roll(total, 512 - 193, 1)
    gb_ref[...] = total[0:6, 0:320]
    rs_finish(2)
    sent("x", xbuf.at[:, pl.ds(0, 2304)])
    sent("h", kext.at[:, pl.ds(0, 512)])
    sent("hb", hb_send)
    sent("c", crecv)
    sent("f", fold)
    sent("u", recv2)
    sent("t", recv3)
    sent("d", dx_send)
    sent("gc", gl_c)
    sent("gr", gl_r)
    assert len(sends) == SENDS and len(recvs) == RECVS, (len(sends), len(recvs))


def write_out(gx, gw, gb, gx_out, gwq_out, gwk_out, gwv_out, gb_out, sem):
    pairs = [(gx, gx_out), (gw.at[0], gwq_out), (gw.at[1], gwk_out), (gw.at[2], gwv_out), (gb, gb_out)]
    copies = [pltpu.make_async_copy(a, b, sem.at[i]) for i, (a, b) in enumerate(pairs)]
    for cp in copies:
        cp.start()
    for cp in copies:
        cp.wait()


def local(inputs, w_query, w_key, w_value, rel_bias, d_out):
    any_spec = pl.BlockSpec(memory_space=pl.ANY)
    vmem = pl.BlockSpec(memory_space=pltpu.VMEM)
    V = pltpu.VMEM
    gx, gw, gb = pl.pallas_call(
        kernel,
        out_shape=(V((512, 768), BF), V((3, 96, 384), F32), V((6, 320), F32)),
        in_specs=[any_spec] * 6,
        out_specs=(vmem, vmem, vmem),
        scratch_shapes=[
            V((512, 3072), BF),
            V((3072, 1152), BF),
            V((4, 768, 512), BF),
            V((2, 3, 128, 384), F32),
            V((3, 768, 128), BF),
            V((3, 768, 128), BF),
            V((3, 512, 128), BF),
            V((512, 384), BF),
            V((3, 128, 768), BF),
            V((3, 768, 128), F32),
            V((3, 768, 128), F32),
            V((3, 384, 256), F32),
            V((3, 384, 256), F32),
            V((512, 1152), BF),
            V((3, 2, 256, 128), BF),
            V((3, 2, 256, 128), BF),
            V((3, 16, 2, 96, 384), BF),
            V((3, 16, 96, 384), BF),
            V((3, 4, 4, 96, 384), BF),
            V((3, 4, 2, 48, 384), BF),
            V((3, 4, 4, 48, 384), BF),
            V((3, 2, 4, 48, 384), BF),
            V((3, 2, 3, 48, 384), BF),
            V((2, 6, 384, 256), BF),
            V((2, 2, 384, 256), BF),
            V((2, 2, 768, 256), BF),
            V((2, 2, 384, 256), BF),
            V((2, 768, 256), BF),
            V((6, 320), F32),
            V((8, 512), F32),
            V((8, 512), F32),
            V((2, 8, 512), F32),
            V((6, 8, 512), F32),
            pltpu.SemaphoreType.DMA,
            pltpu.SemaphoreType.DMA,
            pltpu.SemaphoreType.DMA,
            pltpu.SemaphoreType.DMA,
            pltpu.SemaphoreType.DMA((SENDS,)),
            pltpu.SemaphoreType.DMA((RECVS,)),
        ],
        compiler_params=pltpu.CompilerParams(
            collective_id=0, has_side_effects=True, vmem_limit_bytes=58 * 1024 * 1024
        ),
    )(inputs, w_query, w_key, w_value, rel_bias.T, d_out)
    gx, gwq, gwk, gwv, gb = pl.pallas_call(
        write_out,
        out_shape=(
            jax.ShapeDtypeStruct((512, 768), BF),
            jax.ShapeDtypeStruct((96, 384), F32),
            jax.ShapeDtypeStruct((96, 384), F32),
            jax.ShapeDtypeStruct((96, 384), F32),
            jax.ShapeDtypeStruct((6, 320), F32),
        ),
        in_specs=[vmem] * 3,
        out_specs=[any_spec] * 5,
        scratch_shapes=[pltpu.SemaphoreType.DMA((5,))],
        compiler_params=pltpu.CompilerParams(vmem_limit_bytes=4 * 1024 * 1024),
    )(gx, gw, gb)
    return gx, gwq, gwk, gwv, gb.T


def solution(mesh):
    torus = Mesh(mesh.devices.reshape(4, 4, 2, mesh.shape["tp"]), ("sp_0", "sp_1", "sp_2", "tp"))
    return jax.shard_map(
        local,
        mesh=torus,
        in_specs=(
            P(SP, "tp"),
            P(None, "tp"),
            P(None, "tp"),
            P(None, "tp"),
            P(None, "tp"),
            P(SP, "tp"),
        ),
        out_specs=(P(SP, "tp"), P(SP, "tp"), P(SP, "tp"), P(SP, "tp"), P(None, "tp")),
        check_vma=False,
    )
```

```python
import functools

import jax
import jax.numpy as jnp
from jax import lax
from jax.experimental import pallas as pl
from jax.experimental.pallas import tpu as pltpu
from jax.sharding import Mesh
from jax.sharding import PartitionSpec as P

SP = ("sp_0", "sp_1", "sp_2")
MESH = pl.DeviceIdType.MESH
BF = jnp.bfloat16
F32 = jnp.float32
SENDS, RECVS = 18, 36
LO = 2
CUTS = (0, 384, 896, 1152)

NN = (((1,), (0,)), ((), ()))
NT = (((1,), (1,)), ((), ()))


def dot(a, b, dims=NN):
    return lax.dot_general(a, b, dims, preferred_element_type=F32)


def kernel(
    x_hbm, wq_hbm, wk_hbm, wv_hbm, rb_hbm, do_hbm,
    gx_ref, gw_ref, gb_ref,
    xbuf, w, xt, acc, kext, vext, qs, do, kt, dk_acc, dv_acc, bias, gbias, g,
    hb_send, hb_recv, dwbs, crecvs, s1s, folds, recv2s, s2s, recv3s,
    dx_send, dx_fold, dx_recv, dx_part, dx_own,
    rbuf, gl, gl_c, gl_s, gl_r,
    lsem_x, lsem_b, lsem_w, lsem_do, ssem, rsem,
):
    x = lax.axis_index("tp")
    z = lax.axis_index("sp_0")
    y = lax.axis_index("sp_1")
    c = lax.axis_index("sp_2")
    spi = (z * 4 + y) * 2 + c
    right = {"tp": (x + 1) % 4}
    left = {"tp": (x + 3) % 4}
    nxt = (spi + 1) % 32
    prv = (spi + 31) % 32
    sp_next = {"sp_0": nxt // 8, "sp_1": (nxt // 2) % 4, "sp_2": nxt % 2}
    sp_prev = {"sp_0": prv // 8, "sp_1": (prv // 2) % 4, "sp_2": prv % 2}
    partner = {"sp_2": 1 - c}
    ydev = [None] + [{"sp_1": (y + r) % 4} for r in (1, 2, 3)]
    zdev = [None] + [{"sp_0": (z + r) % 4} for r in (1, 2, 3)]
    yid = [(y + r) % 4 for r in range(4)]
    zid = [(z + r) % 4 for r in range(4)]
    src = [x, (x + 3) % 4, (x + 1) % 4, (x + 2) % 4]

    sends, recvs = {}, {}

    def send(src_ref, dst_ref, dev, out, back):
        pltpu.make_async_remote_copy(
            src_ref=src_ref, dst_ref=dst_ref,
            send_sem=ssem.at[sends.setdefault(out, len(sends))],
            recv_sem=rsem.at[recvs.setdefault(back, len(recvs))],
            device_id=dev, device_id_type=MESH,
        ).start()

    def arrived(back, ref):
        pltpu.make_async_copy(ref, ref, rsem.at[recvs[back]]).wait()

    def sent(out, ref):
        pltpu.make_async_copy(ref, ref, ssem.at[sends[out]]).wait()

    x_copy = pltpu.make_async_copy(x_hbm, xbuf.at[:, pl.ds(0, 768)], lsem_x)
    x_copy.start()
    barrier = pltpu.get_barrier_semaphore()
    peers = [left, right, partner, sp_next, sp_prev] + ydev[1:] + zdev[1:]
    for dev in peers:
        pl.semaphore_signal(barrier, inc=1, device_id=dev, device_id_type=MESH)
    b_copy = pltpu.make_async_copy(rb_hbm, rbuf, lsem_b)
    gl[...] = jnp.zeros_like(gl)
    b_copy.start()
    x_copy.wait()
    pl.semaphore_wait(barrier, len(peers))

    order = (3, 2, 1, 0)
    slot = [pl.ds(768 * i, 768) for i in range(4)]

    def send_own(j):
        rows = pl.ds(128 * j, 128)
        send(xbuf.at[rows, slot[0]], xbuf.at[rows, slot[1]], right, "x", ("xl", j))
        send(xbuf.at[rows, slot[0]], xbuf.at[rows, slot[2]], left, "x", ("xr", j))

    def forward(j):
        rows, first, second = pl.ds(128 * j, 128), pl.ds(128 * j, 64), pl.ds(128 * j + 64, 64)
        arrived(("xl", j), xbuf.at[rows, slot[1]])
        send(xbuf.at[first, slot[1]], xbuf.at[first, slot[3]], right, "x", ("xo", j))
        arrived(("xr", j), xbuf.at[rows, slot[2]])
        send(xbuf.at[second, slot[2]], xbuf.at[second, slot[3]], left, "x", ("xo", j))

    def project_a(j):
        rows = pl.ds(128 * j, 128)

        def body(m, carry):
            cols = pl.ds(pl.multiple_of(m * 384, 128), 384)
            acc[j % 2, m] = dot(xbuf[rows, 0:2304], w[0:2304, cols])
            return carry

        lax.fori_loop(0, 3, body, 0)

    def project_b(j):
        rows = pl.ds(128 * j, 128)
        ext = pl.ds(256 + 128 * j, 128)
        arrived(("xo", j), xbuf.at[rows, slot[3]])
        for m in range(3):
            out = acc[j % 2, m] + dot(xbuf[rows, 2304:3072], w[2304:3072, 384 * m : 384 * m + 384])
            out = out.astype(BF)
            for hp in range(3):
                one = out[:, 128 * hp : 128 * hp + 128]
                if m == 0:
                    qs[hp, rows] = one * jnp.asarray(0.125, BF)
                elif m == 1:
                    kext[hp, ext] = one
                    kt[hp, :, ext] = one.T
                else:
                    vext[hp, ext] = one

    def transpose_rows(j, slots=(0, 1, 2, 3)):
        rows = pl.ds(128 * j, 128)
        for s in slots:
            xt[src[s], :, rows] = xbuf[rows, slot[s]].T

    send_own(order[0])
    send_own(order[1])

    for i in range(4):
        for m, ref in enumerate((wq_hbm, wk_hbm, wv_hbm)):
            pltpu.make_async_copy(
                ref.at[pl.ds(src[i] * 768, 768)], w.at[slot[i], pl.ds(384 * m, 384)], lsem_w
            ).start()
    do_copy = pltpu.make_async_copy(do_hbm, do, lsem_do)
    do_copy.start()

    b_copy.wait()
    gl[0:6, 0:320] = rbuf[...]
    line = pltpu.roll(gl[...], 193, 1)
    lane = lax.broadcasted_iota(jnp.int32, (8, 512), 1)
    line = jnp.where((lane > 0) & (lane < 128), line[:, 0:1], line)
    gl[...] = line
    key_seg = lax.broadcasted_iota(jnp.int32, (384, 128), 0) // 64
    query_seg = lax.broadcasted_iota(jnp.int32, (384, 128), 1) // 64
    seen = (key_seg >= query_seg) & (key_seg <= query_seg + 4)
    for h in range(6):
        wide = jnp.broadcast_to(gl[h : h + 1, :], (384, 512))
        wide = pltpu.roll(wide, 0, 1, stride=1, stride_axis=0)
        bias[h // 2, :, pl.ds(128 * (h % 2), 128)] = jnp.where(seen, wide[:, :128], -jnp.inf)
    gbias[...] = jnp.zeros_like(gbias)
    dk_acc[...] = jnp.zeros_like(dk_acc)
    dv_acc[...] = jnp.zeros_like(dv_acc)

    pltpu.make_async_copy(w, w, lsem_w).wait()
    do_copy.wait()

    forward(order[0])
    send_own(order[2])
    project_a(order[0])
    forward(order[1])
    send_own(order[3])
    project_a(order[1])
    project_b(order[0])
    transpose_rows(order[0])
    forward(order[2])
    project_a(order[2])
    project_b(order[1])
    send(kext.at[:, pl.ds(512, 256)], kext.at[:, pl.ds(0, 256)], sp_next, "h", "hk")
    send(vext.at[:, pl.ds(512, 256)], vext.at[:, pl.ds(0, 256)], sp_next, "h", "hv")
    transpose_rows(order[1])
    transpose_rows(order[2], (0, 1, 2))
    forward(order[3])
    project_a(order[3])
    project_b(order[2])

    lane_q = lax.broadcasted_iota(jnp.int32, (128, 128), 1)
    row_f = lax.broadcasted_iota(jnp.int32, (128, 128), 0)
    zero = jnp.zeros((128, 128), BF)

    def stacked(block):
        return jnp.concatenate(
            [jnp.where(lane_q < 64, block, zero), jnp.where(lane_q >= 64, block, zero)], axis=0
        )

    pen = jnp.where(spi == 0, -jnp.inf, 0.0).astype(F32)

    def unit(hp, qp):
        rows = pl.ds(qp * 128, 128)
        keys = pl.ds(qp * 128, 384)
        qm = stacked(qs[hp, rows])
        dm = stacked(do[rows, 128 * hp : 128 * hp + 128])
        score = dot(kext[hp, keys], qm, NT) + bias[hp]
        if qp < 2:
            cut = 256 - 128 * qp
            score = jnp.concatenate([score[:cut] + pen, score[cut:]], axis=0)
        top = jnp.max(score, axis=0, keepdims=True)
        e = jnp.exp(score - top)
        inv = 1.0 / jnp.sum(e, axis=0, keepdims=True)
        prob = e * inv
        low = prob.astype(BF)
        gp = dot(vext[hp, keys], dm, NT)
        delta = jnp.sum(prob * gp, axis=0, keepdims=True)
        ds = prob * (gp - delta)
        gbias[hp] += ds
        dlow = ds.astype(BF)
        dk_acc[hp, keys] += dot(dlow, qm)
        dv_acc[hp, keys] += dot(low, dm)
        dqt = dot(kt[hp, :, keys], dlow)
        dqt = jnp.where(row_f < 64, dqt[:, :128], dqt[:, 128:]) * 0.125
        g[rows, pl.ds(128 * hp, 128)] = dqt.T.astype(BF)

    def last_units():
        for hp in range(3):
            unit(hp, 3)

    last_units()
    project_b(order[3])
    arrived("hk", kext.at[:, pl.ds(0, 256)])
    arrived("hv", vext.at[:, pl.ds(0, 256)])
    for hp in range(3):
        kt[hp, :, 0:256] = kext[hp, 0:256].T

    def send_halo_grads(heads):
        for hp in heads:
            hb_send[hp, 0] = dk_acc[hp, 0:256].astype(BF)
            hb_send[hp, 1] = dv_acc[hp, 0:256].astype(BF)
        for hp in heads:
            send(hb_send.at[hp], hb_recv.at[hp], sp_prev, "hb", ("hb", hp))

    def attention_first():
        for hp in (0, 1):
            unit(hp, 0)
            unit(hp, 1)
        send_halo_grads((0, 1))

    def attention_rest():
        for hp, qp in ((2, 0), (2, 1), (0, 2), (1, 2), (2, 2)):
            unit(hp, qp)
        for hp in range(3):
            g[0:256, pl.ds(384 + 128 * hp, 128)] = dk_acc[hp, 256:512].astype(BF)
            g[0:256, pl.ds(768 + 128 * hp, 128)] = dv_acc[hp, 256:512].astype(BF)
        send_halo_grads((2,))

    def finish_grads(hp):
        arrived(("hb", hp), hb_recv.at[hp])
        g[256:512, pl.ds(384 + 128 * hp, 128)] = (
            dk_acc[hp, 512:768] + hb_recv[hp, 0].astype(F32)
        ).astype(BF)
        g[256:512, pl.ds(768 + 128 * hp, 128)] = (
            dv_acc[hp, 512:768] + hb_recv[hp, 1].astype(F32)
        ).astype(BF)

    def weight_grad(m):
        dwb, crecv = dwbs[m], crecvs[m]
        width = CUTS[m + 1] - CUTS[m]
        step = 1 if width > 256 else 2
        for first in range(0, 4, step):
            blocks = range(first, first + step)
            outs = [dot(xt[i], g[:, CUTS[m] : CUTS[m + 1]]).astype(BF) for i in blocks]
            for i, out in zip(blocks, outs):
                dwb[4 * i : 4 * i + 4] = out.reshape(4, 2, 96, width)
            part = pl.ds(4 * first, 4 * step)
            send(dwb.at[part, 1 - c], crecv.at[part], partner, ("c", m), ("c", m))

    lo, hi = pl.ds(0, LO), pl.ds(LO, 4 - LO)
    ra, rb = pl.ds(0, 48), pl.ds(48, 48)

    def rs_start(m):
        dwb, crecv, s1, fold, recv2 = dwbs[m], crecvs[m], s1s[m], folds[m], recv2s[m]
        arrived(("c", m), crecv)

        def body(i, carry):
            zz, yy = i // 4, i % 4
            s1[zz, yy] = (dwb[i, c].astype(F32) + crecv[i].astype(F32)).astype(BF)
            return carry

        lax.fori_loop(0, 16, body, 0)
        f, u = ("f", m), ("u", m)
        send(s1.at[lo, yid[2], ra], fold.at[0, lo], ydev[1], f, f)
        send(s1.at[hi, yid[2], ra], fold.at[0, hi], ydev[3], f, f)
        send(s1.at[zid[2], lo, rb], fold.at[1, lo], zdev[1], f, f)
        send(s1.at[zid[2], hi, rb], fold.at[1, hi], zdev[3], f, f)
        send(s1.at[hi, yid[1], ra], recv2.at[0, hi], ydev[1], u, u)
        send(s1.at[lo, yid[3], ra], recv2.at[1, lo], ydev[3], u, u)
        send(s1.at[zid[1], hi, rb], recv2.at[2, hi], zdev[1], u, u)
        send(s1.at[zid[3], lo, rb], recv2.at[3, lo], zdev[3], u, u)

    def rs_fold(m):
        s1, fold, recv2 = s1s[m], folds[m], recv2s[m]
        u = ("u", m)
        arrived(("f", m), fold)
        for i in range(4):
            r = 1 if i < LO else 3
            for part, at in enumerate(((i, yid[r], ra), (zid[r], i, rb))):
                s1[at] = (s1[at].astype(F32) + fold[part, i].astype(F32)).astype(BF)
        send(s1.at[lo, yid[1], ra], recv2.at[0, lo], ydev[1], u, u)
        send(s1.at[hi, yid[3], ra], recv2.at[1, hi], ydev[3], u, u)
        send(s1.at[zid[1], lo, rb], recv2.at[2, lo], zdev[1], u, u)
        send(s1.at[zid[3], hi, rb], recv2.at[3, hi], zdev[3], u, u)

    def rs_second(m):
        s1, recv2, s2, recv3 = s1s[m], recv2s[m], s2s[m], recv3s[m]
        arrived(("u", m), recv2)
        for i in range(4):
            s2[0, i] = (
                s1[i, y, ra].astype(F32) + recv2[0, i].astype(F32) + recv2[1, i].astype(F32)
            ).astype(BF)
            s2[1, i] = (
                s1[z, i, rb].astype(F32) + recv2[2, i].astype(F32) + recv2[3, i].astype(F32)
            ).astype(BF)
        for r in (1, 3, 2):
            send(s2.at[0, zid[r]], recv3.at[0, r - 1], zdev[r], ("t", m), ("t", m))
            send(s2.at[1, yid[r]], recv3.at[1, r - 1], ydev[r], ("t", m), ("t", m))

    def rs_finish(m):
        s2, recv3 = s2s[m], recv3s[m]
        arrived(("t", m), recv3)
        for part, own in ((0, z), (1, y)):
            total = s2[part, own].astype(F32)
            for r in range(3):
                total += recv3[part, r].astype(F32)
            gw_ref[pl.ds(48 * part, 48), CUTS[m] : CUTS[m + 1]] = total

    def dx_block(t, s, start=0, size=768):
        rows = slice(768 * s + start, 768 * s + start + size)
        return dot(w[rows, :], g[256 * t : 256 * t + 256, :], NT).astype(BF)

    half_a, half_b = pl.ds(0, 384), pl.ds(384, 384)

    def dx_opposite(t):
        first, second = dx_block(t, 3, 0, 384), dx_block(t, 3, 384, 384)
        dx_send[t, 0] = first
        dx_send[t, 1] = second
        send(dx_send.at[t, 0], dx_fold.at[t, 0], right, "d", ("df", t))
        send(dx_send.at[t, 1], dx_fold.at[t, 1], left, "d", ("df", t))

    def dx_direct(t):
        for_right, for_left = dx_block(t, 2), dx_block(t, 1)
        dx_send[t, 2] = for_right[384:]
        dx_part[t, 0] = for_right[:384]
        dx_send[t, 3] = for_left[:384]
        dx_part[t, 1] = for_left[384:]
        send(dx_send.at[t, 2], dx_recv.at[t, 0, half_b], right, "d", ("d", t))
        send(dx_send.at[t, 3], dx_recv.at[t, 1, half_a], left, "d", ("d", t))

    def dx_folded(t):
        arrived(("df", t), dx_fold.at[t])
        dx_send[t, 4] = (dx_part[t, 0].astype(F32) + dx_fold[t, 0].astype(F32)).astype(BF)
        dx_send[t, 5] = (dx_part[t, 1].astype(F32) + dx_fold[t, 1].astype(F32)).astype(BF)
        send(dx_send.at[t, 4], dx_recv.at[t, 0, half_a], right, "d", ("d", t))
        send(dx_send.at[t, 5], dx_recv.at[t, 1, half_b], left, "d", ("d", t))

    def dx_mine():
        first, second = dx_block(0, 0), dx_block(1, 0)
        dx_own[0] = first
        dx_own[1] = second

    def dx_finish(t):
        arrived(("d", t), dx_recv.at[t])
        total = (
            dx_own[t].astype(F32) + dx_recv[t, 0].astype(F32) + dx_recv[t, 1].astype(F32)
        )
        gx_ref[pl.ds(256 * t, 256), :] = total.T.astype(BF)

    def bias_line():
        for hp in range(3):
            for par in range(2):
                total = jnp.zeros((8, 512), F32)
                for a in range(48):
                    part = gbias[hp, pl.ds(8 * a, 8), pl.ds(128 * par, 128)]
                    part = jnp.concatenate([part, jnp.zeros((8, 384), F32)], axis=1)
                    total += pltpu.roll(part, (512 - 8 * a) % 512, 1)
                sub = lax.broadcasted_iota(jnp.int32, (8, 512), 0)
                for bit in range(3):
                    moved = pltpu.roll(total, 512 - (1 << bit), 1)
                    total = jnp.where((sub >> bit) % 2 == 1, moved, total)
                h = 2 * hp + par
                gl[h : h + 1, :] = jnp.sum(total, axis=0, keepdims=True)
        gl[6:8, :] = jnp.zeros((2, 512), F32)

    attention_first()
    attention_rest()
    dx_opposite(0)
    transpose_rows(order[2], (3,))
    transpose_rows(order[3])
    weight_grad(0)
    dx_direct(0)
    rs_start(0)
    finish_grads(0)
    finish_grads(1)
    finish_grads(2)
    weight_grad(1)
    dx_opposite(1)
    dx_folded(0)
    rs_fold(0)
    rs_start(1)
    weight_grad(2)
    dx_direct(1)
    rs_start(2)
    bias_line()
    send(gl, gl_c, partner, "gc", "gc")
    rs_second(0)
    rs_fold(1)
    arrived("gc", gl_c)
    gl_s[0] = gl[...] + gl_c[...]
    for r in (1, 2, 3):
        send(gl_s.at[0], gl_r.at[r - 1], ydev[r], "gr", "gy")
    dx_folded(1)
    dx_mine()
    rs_fold(2)
    dx_finish(0)
    rs_second(1)
    rs_second(2)
    arrived("gy", gl_r.at[pl.ds(0, 3)])
    gl_s[1] = gl_s[0] + gl_r[0] + gl_r[1] + gl_r[2]
    for r in (1, 2, 3):
        send(gl_s.at[1], gl_r.at[2 + r], zdev[r], "gr", "gz")
    rs_finish(0)
    dx_finish(1)
    rs_finish(1)
    arrived("gz", gl_r.at[pl.ds(3, 3)])
    total = gl_s[1] + gl_r[3] + gl_r[4] + gl_r[5]
    far = jnp.sum(jnp.where(lane < 128, total, 0.0), axis=1, keepdims=True)
    total = jnp.where(lane == 0, far, total)
    total = pltpu.roll(total, 512 - 193, 1)
    gb_ref[...] = total[0:6, 0:320]
    rs_finish(2)
    sent("x", xbuf.at[:, pl.ds(0, 2304)])
    sent("h", kext.at[:, pl.ds(0, 512)])
    sent("hb", hb_send)
    for m in range(3):
        sent(("c", m), crecvs[m])
        sent(("f", m), folds[m])
        sent(("u", m), recv2s[m])
        sent(("t", m), recv3s[m])
    sent("d", dx_send)
    sent("gc", gl_c)
    sent("gr", gl_r)
    assert len(sends) == SENDS and len(recvs) == RECVS, (len(sends), len(recvs))


def write_out(gx, gw, gb, gx_out, gwq_out, gwk_out, gwv_out, gb_out, sem):
    gws = [gw.at[:, pl.ds(384 * m, 384)] for m in range(3)]
    pairs = [(gx, gx_out), (gws[0], gwq_out), (gws[1], gwk_out), (gws[2], gwv_out), (gb, gb_out)]
    copies = [pltpu.make_async_copy(a, b, sem.at[i]) for i, (a, b) in enumerate(pairs)]
    for cp in copies:
        cp.start()
    for cp in copies:
        cp.wait()


def local(inputs, w_query, w_key, w_value, rel_bias, d_out):
    any_spec = pl.BlockSpec(memory_space=pl.ANY)
    vmem = pl.BlockSpec(memory_space=pltpu.VMEM)
    V = pltpu.VMEM

    def per_cut(*dims):
        return tuple(V((*dims, b - a), BF) for a, b in zip(CUTS, CUTS[1:]))

    gx, gw, gb = pl.pallas_call(
        kernel,
        out_shape=(V((512, 768), BF), V((96, 1152), F32), V((6, 320), F32)),
        in_specs=[any_spec] * 6,
        out_specs=(vmem, vmem, vmem),
        scratch_shapes=[
            V((512, 3072), BF),
            V((3072, 1152), BF),
            V((4, 768, 512), BF),
            V((2, 3, 128, 384), F32),
            V((3, 768, 128), BF),
            V((3, 768, 128), BF),
            V((3, 512, 128), BF),
            V((512, 384), BF),
            V((3, 128, 768), BF),
            V((3, 768, 128), F32),
            V((3, 768, 128), F32),
            V((3, 384, 256), F32),
            V((3, 384, 256), F32),
            V((512, 1152), BF),
            V((3, 2, 256, 128), BF),
            V((3, 2, 256, 128), BF),
            per_cut(16, 2, 96),
            per_cut(16, 96),
            per_cut(4, 4, 96),
            per_cut(2, 4, 48),
            per_cut(4, 4, 48),
            per_cut(2, 4, 48),
            per_cut(2, 3, 48),
            V((2, 6, 384, 256), BF),
            V((2, 2, 384, 256), BF),
            V((2, 2, 768, 256), BF),
            V((2, 2, 384, 256), BF),
            V((2, 768, 256), BF),
            V((6, 320), F32),
            V((8, 512), F32),
            V((8, 512), F32),
            V((2, 8, 512), F32),
            V((6, 8, 512), F32),
            pltpu.SemaphoreType.DMA,
            pltpu.SemaphoreType.DMA,
            pltpu.SemaphoreType.DMA,
            pltpu.SemaphoreType.DMA,
            pltpu.SemaphoreType.DMA((SENDS,)),
            pltpu.SemaphoreType.DMA((RECVS,)),
        ],
        compiler_params=pltpu.CompilerParams(
            collective_id=0, has_side_effects=True, vmem_limit_bytes=58 * 1024 * 1024
        ),
    )(inputs, w_query, w_key, w_value, rel_bias.T, d_out)
    gx, gwq, gwk, gwv, gb = pl.pallas_call(
        write_out,
        out_shape=(
            jax.ShapeDtypeStruct((512, 768), BF),
            jax.ShapeDtypeStruct((96, 384), F32),
            jax.ShapeDtypeStruct((96, 384), F32),
            jax.ShapeDtypeStruct((96, 384), F32),
            jax.ShapeDtypeStruct((6, 320), F32),
        ),
        in_specs=[vmem] * 3,
        out_specs=[any_spec] * 5,
        scratch_shapes=[pltpu.SemaphoreType.DMA((5,))],
        compiler_params=pltpu.CompilerParams(vmem_limit_bytes=4 * 1024 * 1024),
    )(gx, gw, gb)
    return gx, gwq, gwk, gwv, gb.T


def solution(mesh):
    torus = Mesh(mesh.devices.reshape(4, 4, 2, mesh.shape["tp"]), ("sp_0", "sp_1", "sp_2", "tp"))
    return jax.shard_map(
        local,
        mesh=torus,
        in_specs=(
            P(SP, "tp"),
            P(None, "tp"),
            P(None, "tp"),
            P(None, "tp"),
            P(None, "tp"),
            P(SP, "tp"),
        ),
        out_specs=(P(SP, "tp"), P(SP, "tp"), P(SP, "tp"), P(SP, "tp"), P(None, "tp")),
        check_vma=False,
    )
```

```python
import functools

import jax
import jax.numpy as jnp
from jax import lax
from jax.experimental import pallas as pl
from jax.experimental.pallas import tpu as pltpu
from jax.sharding import Mesh
from jax.sharding import PartitionSpec as P

SP = ("sp_0", "sp_1", "sp_2")
MESH = pl.DeviceIdType.MESH
BF = jnp.bfloat16
F32 = jnp.float32
SENDS, RECVS = 18, 36
LO = 2
CUTS = (0, 384, 896, 1152)

NN = (((1,), (0,)), ((), ()))
NT = (((1,), (1,)), ((), ()))


def dot(a, b, dims=NN):
    return lax.dot_general(a, b, dims, preferred_element_type=F32)


def kernel(
    x_hbm, wq_hbm, wk_hbm, wv_hbm, rb_hbm, do_hbm,
    gx_ref, gw_ref, gb_ref,
    xbuf, w, xt, acc, kext, vext, qs, do, kt, dk_acc, dv_acc, bias, gbias, g,
    hb_send, hb_recv, dwbs, crecvs, s1s, folds, recv2s, s2s, recv3s,
    dx_send, dx_fold, dx_recv, dx_part, dx_own,
    rbuf, gl, gl_c, gl_s, gl_r,
    lsem_x, lsem_b, lsem_w, lsem_do, ssem, rsem,
):
    x = lax.axis_index("tp")
    z = lax.axis_index("sp_0")
    y = lax.axis_index("sp_1")
    c = lax.axis_index("sp_2")
    spi = (z * 4 + y) * 2 + c
    right = {"tp": (x + 1) % 4}
    left = {"tp": (x + 3) % 4}
    nxt = (spi + 1) % 32
    prv = (spi + 31) % 32
    sp_next = {"sp_0": nxt // 8, "sp_1": (nxt // 2) % 4, "sp_2": nxt % 2}
    sp_prev = {"sp_0": prv // 8, "sp_1": (prv // 2) % 4, "sp_2": prv % 2}
    partner = {"sp_2": 1 - c}
    ydev = [None] + [{"sp_1": (y + r) % 4} for r in (1, 2, 3)]
    zdev = [None] + [{"sp_0": (z + r) % 4} for r in (1, 2, 3)]
    yid = [(y + r) % 4 for r in range(4)]
    zid = [(z + r) % 4 for r in range(4)]
    src = [x, (x + 3) % 4, (x + 1) % 4, (x + 2) % 4]

    sends, recvs = {}, {}

    def send(src_ref, dst_ref, dev, out, back):
        pltpu.make_async_remote_copy(
            src_ref=src_ref, dst_ref=dst_ref,
            send_sem=ssem.at[sends.setdefault(out, len(sends))],
            recv_sem=rsem.at[recvs.setdefault(back, len(recvs))],
            device_id=dev, device_id_type=MESH,
        ).start()

    def arrived(back, ref):
        pltpu.make_async_copy(ref, ref, rsem.at[recvs[back]]).wait()

    def sent(out, ref):
        pltpu.make_async_copy(ref, ref, ssem.at[sends[out]]).wait()

    x_copy = pltpu.make_async_copy(x_hbm, xbuf.at[:, pl.ds(0, 768)], lsem_x)
    x_copy.start()
    barrier = pltpu.get_barrier_semaphore()
    peers = [left, right, partner, sp_next, sp_prev] + ydev[1:] + zdev[1:]
    for dev in peers:
        pl.semaphore_signal(barrier, inc=1, device_id=dev, device_id_type=MESH)
    b_copy = pltpu.make_async_copy(rb_hbm, rbuf, lsem_b)
    gl[...] = jnp.zeros_like(gl)
    b_copy.start()
    x_copy.wait()
    pl.semaphore_wait(barrier, len(peers))

    order = (3, 2, 1, 0)
    slot = [pl.ds(768 * i, 768) for i in range(4)]

    def send_own(j):
        rows = pl.ds(128 * j, 128)
        send(xbuf.at[rows, slot[0]], xbuf.at[rows, slot[1]], right, "x", ("xl", j))
        send(xbuf.at[rows, slot[0]], xbuf.at[rows, slot[2]], left, "x", ("xr", j))

    def forward(j):
        rows, first, second = pl.ds(128 * j, 128), pl.ds(128 * j, 64), pl.ds(128 * j + 64, 64)
        arrived(("xl", j), xbuf.at[rows, slot[1]])
        send(xbuf.at[first, slot[1]], xbuf.at[first, slot[3]], right, "x", ("xo", j))
        arrived(("xr", j), xbuf.at[rows, slot[2]])
        send(xbuf.at[second, slot[2]], xbuf.at[second, slot[3]], left, "x", ("xo", j))

    def project_a(j):
        rows = pl.ds(128 * j, 128)

        def body(m, carry):
            cols = pl.ds(pl.multiple_of(m * 384, 128), 384)
            acc[j % 2, m] = dot(xbuf[rows, 0:2304], w[0:2304, cols])
            return carry

        lax.fori_loop(0, 3, body, 0)

    def project_b(j):
        rows = pl.ds(128 * j, 128)
        ext = pl.ds(256 + 128 * j, 128)
        arrived(("xo", j), xbuf.at[rows, slot[3]])
        for m in range(3):
            out = acc[j % 2, m] + dot(xbuf[rows, 2304:3072], w[2304:3072, 384 * m : 384 * m + 384])
            out = out.astype(BF)
            for hp in range(3):
                one = out[:, 128 * hp : 128 * hp + 128]
                if m == 0:
                    qs[hp, rows] = one * jnp.asarray(0.125, BF)
                elif m == 1:
                    kext[hp, ext] = one
                    kt[hp, :, ext] = one.T
                else:
                    vext[hp, ext] = one

    def transpose_rows(j, slots=(0, 1, 2, 3)):
        rows = pl.ds(128 * j, 128)
        for s in slots:
            xt[src[s], :, rows] = xbuf[rows, slot[s]].T

    send_own(order[0])
    send_own(order[1])

    for i in range(4):
        for m, ref in enumerate((wq_hbm, wk_hbm, wv_hbm)):
            pltpu.make_async_copy(
                ref.at[pl.ds(src[i] * 768, 768)], w.at[slot[i], pl.ds(384 * m, 384)], lsem_w
            ).start()
    do_copy = pltpu.make_async_copy(do_hbm, do, lsem_do)
    do_copy.start()

    b_copy.wait()
    gl[0:6, 0:320] = rbuf[...]
    line = pltpu.roll(gl[...], 193, 1)
    lane = lax.broadcasted_iota(jnp.int32, (8, 512), 1)
    line = jnp.where((lane > 0) & (lane < 128), line[:, 0:1], line)
    gl[...] = line
    key_seg = lax.broadcasted_iota(jnp.int32, (384, 128), 0) // 64
    query_seg = lax.broadcasted_iota(jnp.int32, (384, 128), 1) // 64
    seen = (key_seg >= query_seg) & (key_seg <= query_seg + 4)
    for h in range(6):
        wide = jnp.broadcast_to(gl[h : h + 1, :], (384, 512))
        wide = pltpu.roll(wide, 0, 1, stride=1, stride_axis=0)
        bias[h // 2, :, pl.ds(128 * (h % 2), 128)] = jnp.where(seen, wide[:, :128], -jnp.inf)
    gbias[...] = jnp.zeros_like(gbias)
    dk_acc[...] = jnp.zeros_like(dk_acc)
    dv_acc[...] = jnp.zeros_like(dv_acc)

    pltpu.make_async_copy(w, w, lsem_w).wait()
    do_copy.wait()

    forward(order[0])
    send_own(order[2])
    project_a(order[0])
    forward(order[1])
    send_own(order[3])
    project_a(order[1])
    project_b(order[0])
    transpose_rows(order[0])
    forward(order[2])
    project_a(order[2])
    project_b(order[1])
    send(kext.at[:, pl.ds(512, 256)], kext.at[:, pl.ds(0, 256)], sp_next, "h", "hk")
    send(vext.at[:, pl.ds(512, 256)], vext.at[:, pl.ds(0, 256)], sp_next, "h", "hv")
    transpose_rows(order[1])
    transpose_rows(order[2], (0, 1, 2))
    forward(order[3])
    project_a(order[3])
    project_b(order[2])

    lane_q = lax.broadcasted_iota(jnp.int32, (128, 128), 1)
    row_f = lax.broadcasted_iota(jnp.int32, (128, 128), 0)
    zero = jnp.zeros((128, 128), BF)

    def stacked(block):
        return jnp.concatenate(
            [jnp.where(lane_q < 64, block, zero), jnp.where(lane_q >= 64, block, zero)], axis=0
        )

    pen = jnp.where(spi == 0, -jnp.inf, 0.0).astype(F32)

    def unit(hp, qp):
        rows = pl.ds(qp * 128, 128)
        keys = pl.ds(qp * 128, 384)
        qm = stacked(qs[hp, rows])
        dm = stacked(do[rows, 128 * hp : 128 * hp + 128])
        score = dot(kext[hp, keys], qm, NT) + bias[hp]
        if qp < 2:
            cut = 256 - 128 * qp
            score = jnp.concatenate([score[:cut] + pen, score[cut:]], axis=0)
        top = jnp.max(score, axis=0, keepdims=True)
        e = jnp.exp(score - top)
        inv = 1.0 / jnp.sum(e, axis=0, keepdims=True)
        prob = e * inv
        low = prob.astype(BF)
        gp = dot(vext[hp, keys], dm, NT)
        delta = jnp.sum(prob * gp, axis=0, keepdims=True)
        ds = prob * (gp - delta)
        gbias[hp] += ds
        dlow = ds.astype(BF)
        dk_acc[hp, keys] += dot(dlow, qm)
        dv_acc[hp, keys] += dot(low, dm)
        dqt = dot(kt[hp, :, keys], dlow)
        dqt = jnp.where(row_f < 64, dqt[:, :128], dqt[:, 128:]) * 0.125
        g[rows, pl.ds(128 * hp, 128)] = dqt.T.astype(BF)

    def last_units():
        for hp in range(3):
            unit(hp, 3)

    last_units()
    project_b(order[3])
    arrived("hk", kext.at[:, pl.ds(0, 256)])
    arrived("hv", vext.at[:, pl.ds(0, 256)])
    for hp in range(3):
        kt[hp, :, 0:256] = kext[hp, 0:256].T

    def send_halo_grads(heads):
        for hp in heads:
            hb_send[hp, 0] = dk_acc[hp, 0:256].astype(BF)
            hb_send[hp, 1] = dv_acc[hp, 0:256].astype(BF)
        for hp in heads:
            send(hb_send.at[hp], hb_recv.at[hp], sp_prev, "hb", ("hb", hp))

    def attention_first():
        for hp in (0, 1):
            unit(hp, 0)
            unit(hp, 1)
        send_halo_grads((0, 1))

    def attention_rest():
        for hp, qp in ((2, 0), (2, 1), (0, 2), (1, 2), (2, 2)):
            unit(hp, qp)
        for hp in range(3):
            g[0:256, pl.ds(384 + 128 * hp, 128)] = dk_acc[hp, 256:512].astype(BF)
            g[0:256, pl.ds(768 + 128 * hp, 128)] = dv_acc[hp, 256:512].astype(BF)
        send_halo_grads((2,))

    def finish_grads(hp):
        arrived(("hb", hp), hb_recv.at[hp])
        g[256:512, pl.ds(384 + 128 * hp, 128)] = (
            dk_acc[hp, 512:768] + hb_recv[hp, 0].astype(F32)
        ).astype(BF)
        g[256:512, pl.ds(768 + 128 * hp, 128)] = (
            dv_acc[hp, 512:768] + hb_recv[hp, 1].astype(F32)
        ).astype(BF)

    def weight_grad(m):
        dwb, crecv = dwbs[m], crecvs[m]
        width = CUTS[m + 1] - CUTS[m]
        step = 1 if width > 256 else 2
        for first in range(0, 4, step):
            blocks = range(first, first + step)
            outs = [dot(xt[i], g[:, CUTS[m] : CUTS[m + 1]]).astype(BF) for i in blocks]
            for i, out in zip(blocks, outs):
                dwb[4 * i : 4 * i + 4] = out.reshape(4, 2, 96, width)
            part = pl.ds(4 * first, 4 * step)
            send(dwb.at[part, 1 - c], crecv.at[part], partner, ("c", m), ("c", m))

    lo, hi = pl.ds(0, LO), pl.ds(LO, 4 - LO)
    ra, rb = pl.ds(0, 48), pl.ds(48, 48)

    def rs_start(m):
        dwb, crecv, s1, fold, recv2 = dwbs[m], crecvs[m], s1s[m], folds[m], recv2s[m]
        arrived(("c", m), crecv)

        def body(i, carry):
            zz, yy = i // 4, i % 4
            s1[zz, yy] = dwb[i, c] + crecv[i]
            return carry

        lax.fori_loop(0, 16, body, 0, unroll=2)
        f, u = ("f", m), ("u", m)
        send(s1.at[lo, yid[2], ra], fold.at[0, lo], ydev[1], f, f)
        send(s1.at[hi, yid[2], ra], fold.at[0, hi], ydev[3], f, f)
        send(s1.at[zid[2], lo, rb], fold.at[1, lo], zdev[1], f, f)
        send(s1.at[zid[2], hi, rb], fold.at[1, hi], zdev[3], f, f)
        send(s1.at[hi, yid[1], ra], recv2.at[0, hi], ydev[1], u, u)
        send(s1.at[lo, yid[3], ra], recv2.at[1, lo], ydev[3], u, u)
        send(s1.at[zid[1], hi, rb], recv2.at[2, hi], zdev[1], u, u)
        send(s1.at[zid[3], lo, rb], recv2.at[3, lo], zdev[3], u, u)

    def rs_fold(m):
        s1, fold, recv2 = s1s[m], folds[m], recv2s[m]
        u = ("u", m)
        arrived(("f", m), fold)
        for i in range(4):
            r = 1 if i < LO else 3
            for part, at in enumerate(((i, yid[r], ra), (zid[r], i, rb))):
                s1[at] = s1[at] + fold[part, i]
        send(s1.at[lo, yid[1], ra], recv2.at[0, lo], ydev[1], u, u)
        send(s1.at[hi, yid[3], ra], recv2.at[1, hi], ydev[3], u, u)
        send(s1.at[zid[1], lo, rb], recv2.at[2, lo], zdev[1], u, u)
        send(s1.at[zid[3], hi, rb], recv2.at[3, hi], zdev[3], u, u)

    def rs_second(m):
        s1, recv2, s2, recv3 = s1s[m], recv2s[m], s2s[m], recv3s[m]
        arrived(("u", m), recv2)
        for i in range(4):
            s2[0, i] = (
                s1[i, y, ra].astype(F32) + recv2[0, i].astype(F32) + recv2[1, i].astype(F32)
            ).astype(BF)
            s2[1, i] = (
                s1[z, i, rb].astype(F32) + recv2[2, i].astype(F32) + recv2[3, i].astype(F32)
            ).astype(BF)
        for r in (1, 3, 2):
            send(s2.at[0, zid[r]], recv3.at[0, r - 1], zdev[r], ("t", m), ("t", m))
            send(s2.at[1, yid[r]], recv3.at[1, r - 1], ydev[r], ("t", m), ("t", m))

    def rs_finish(m):
        s2, recv3 = s2s[m], recv3s[m]
        arrived(("t", m), recv3)
        for part, own in ((0, z), (1, y)):
            total = s2[part, own].astype(F32)
            for r in range(3):
                total += recv3[part, r].astype(F32)
            gw_ref[pl.ds(48 * part, 48), CUTS[m] : CUTS[m + 1]] = total

    def dx_block(t, s, start=0, size=768):
        rows = slice(768 * s + start, 768 * s + start + size)
        return dot(w[rows, :], g[256 * t : 256 * t + 256, :], NT).astype(BF)

    half_a, half_b = pl.ds(0, 384), pl.ds(384, 384)

    def dx_opposite(t):
        first, second = dx_block(t, 3, 0, 384), dx_block(t, 3, 384, 384)
        dx_send[t, 0] = first
        dx_send[t, 1] = second
        send(dx_send.at[t, 0], dx_fold.at[t, 0], right, "d", ("df", t))
        send(dx_send.at[t, 1], dx_fold.at[t, 1], left, "d", ("df", t))

    def dx_direct(t):
        for_right, for_left = dx_block(t, 2), dx_block(t, 1)
        dx_send[t, 2] = for_right[384:]
        dx_part[t, 0] = for_right[:384]
        dx_send[t, 3] = for_left[:384]
        dx_part[t, 1] = for_left[384:]
        send(dx_send.at[t, 2], dx_recv.at[t, 0, half_b], right, "d", ("d", t))
        send(dx_send.at[t, 3], dx_recv.at[t, 1, half_a], left, "d", ("d", t))

    def dx_folded(t):
        arrived(("df", t), dx_fold.at[t])
        dx_send[t, 4] = dx_part[t, 0] + dx_fold[t, 0]
        dx_send[t, 5] = dx_part[t, 1] + dx_fold[t, 1]
        send(dx_send.at[t, 4], dx_recv.at[t, 0, half_a], right, "d", ("d", t))
        send(dx_send.at[t, 5], dx_recv.at[t, 1, half_b], left, "d", ("d", t))

    def dx_mine():
        first, second = dx_block(0, 0), dx_block(1, 0)
        dx_own[0] = first
        dx_own[1] = second

    def dx_finish(t):
        arrived(("d", t), dx_recv.at[t])
        total = (
            dx_own[t].astype(F32) + dx_recv[t, 0].astype(F32) + dx_recv[t, 1].astype(F32)
        )
        gx_ref[pl.ds(256 * t, 256), :] = total.T.astype(BF)

    def bias_line():
        for hp in range(3):
            for par in range(2):
                total = jnp.zeros((8, 512), F32)
                for a in range(48):
                    part = gbias[hp, pl.ds(8 * a, 8), pl.ds(128 * par, 128)]
                    part = jnp.concatenate([part, jnp.zeros((8, 384), F32)], axis=1)
                    total += pltpu.roll(part, (512 - 8 * a) % 512, 1)
                sub = lax.broadcasted_iota(jnp.int32, (8, 512), 0)
                for bit in range(3):
                    moved = pltpu.roll(total, 512 - (1 << bit), 1)
                    total = jnp.where((sub >> bit) % 2 == 1, moved, total)
                h = 2 * hp + par
                gl[h : h + 1, :] = jnp.sum(total, axis=0, keepdims=True)
        gl[6:8, :] = jnp.zeros((2, 512), F32)

    attention_first()
    attention_rest()
    dx_opposite(0)
    transpose_rows(order[2], (3,))
    transpose_rows(order[3])
    weight_grad(0)
    dx_direct(0)
    rs_start(0)
    finish_grads(0)
    finish_grads(1)
    finish_grads(2)
    weight_grad(1)
    dx_opposite(1)
    dx_folded(0)
    rs_fold(0)
    rs_start(1)
    weight_grad(2)
    dx_direct(1)
    bias_line()
    send(gl, gl_c, partner, "gc", "gc")
    rs_start(2)
    rs_second(0)
    arrived("gc", gl_c)
    gl_s[0] = gl[...] + gl_c[...]
    for r in (1, 2, 3):
        send(gl_s.at[0], gl_r.at[r - 1], ydev[r], "gr", "gy")
    rs_fold(1)
    dx_folded(1)
    dx_mine()
    rs_fold(2)
    dx_finish(0)
    arrived("gy", gl_r.at[pl.ds(0, 3)])
    gl_s[1] = gl_s[0] + gl_r[0] + gl_r[1] + gl_r[2]
    for r in (1, 2, 3):
        send(gl_s.at[1], gl_r.at[2 + r], zdev[r], "gr", "gz")
    rs_second(1)
    rs_second(2)
    rs_finish(0)
    arrived("gz", gl_r.at[pl.ds(3, 3)])
    total = gl_s[1] + gl_r[3] + gl_r[4] + gl_r[5]
    far = jnp.sum(jnp.where(lane < 128, total, 0.0), axis=1, keepdims=True)
    total = jnp.where(lane == 0, far, total)
    total = pltpu.roll(total, 512 - 193, 1)
    gb_ref[...] = total[0:6, 0:320]
    rs_finish(1)
    dx_finish(1)
    rs_finish(2)
    sent("x", xbuf.at[:, pl.ds(0, 2304)])
    sent("h", kext.at[:, pl.ds(0, 512)])
    sent("hb", hb_send)
    for m in range(3):
        sent(("c", m), crecvs[m])
        sent(("f", m), folds[m])
        sent(("u", m), recv2s[m])
        sent(("t", m), recv3s[m])
    sent("d", dx_send)
    sent("gc", gl_c)
    sent("gr", gl_r)
    assert len(sends) == SENDS and len(recvs) == RECVS, (len(sends), len(recvs))


def write_out(gx, gw, gb, gx_out, gwq_out, gwk_out, gwv_out, gb_out, sem):
    gws = [gw.at[:, pl.ds(384 * m, 384)] for m in range(3)]
    pairs = [(gx, gx_out), (gws[0], gwq_out), (gws[1], gwk_out), (gws[2], gwv_out), (gb, gb_out)]
    copies = [pltpu.make_async_copy(a, b, sem.at[i]) for i, (a, b) in enumerate(pairs)]
    for cp in copies:
        cp.start()
    for cp in copies:
        cp.wait()


def local(inputs, w_query, w_key, w_value, rel_bias, d_out):
    any_spec = pl.BlockSpec(memory_space=pl.ANY)
    vmem = pl.BlockSpec(memory_space=pltpu.VMEM)
    V = pltpu.VMEM

    def per_cut(*dims):
        return tuple(V((*dims, b - a), BF) for a, b in zip(CUTS, CUTS[1:]))

    gx, gw, gb = pl.pallas_call(
        kernel,
        out_shape=(V((512, 768), BF), V((96, 1152), F32), V((6, 320), F32)),
        in_specs=[any_spec] * 6,
        out_specs=(vmem, vmem, vmem),
        scratch_shapes=[
            V((512, 3072), BF),
            V((3072, 1152), BF),
            V((4, 768, 512), BF),
            V((2, 3, 128, 384), F32),
            V((3, 768, 128), BF),
            V((3, 768, 128), BF),
            V((3, 512, 128), BF),
            V((512, 384), BF),
            V((3, 128, 768), BF),
            V((3, 768, 128), F32),
            V((3, 768, 128), F32),
            V((3, 384, 256), F32),
            V((3, 384, 256), F32),
            V((512, 1152), BF),
            V((3, 2, 256, 128), BF),
            V((3, 2, 256, 128), BF),
            per_cut(16, 2, 96),
            per_cut(16, 96),
            per_cut(4, 4, 96),
            per_cut(2, 4, 48),
            per_cut(4, 4, 48),
            per_cut(2, 4, 48),
            per_cut(2, 3, 48),
            V((2, 6, 384, 256), BF),
            V((2, 2, 384, 256), BF),
            V((2, 2, 768, 256), BF),
            V((2, 2, 384, 256), BF),
            V((2, 768, 256), BF),
            V((6, 320), F32),
            V((8, 512), F32),
            V((8, 512), F32),
            V((2, 8, 512), F32),
            V((6, 8, 512), F32),
            pltpu.SemaphoreType.DMA,
            pltpu.SemaphoreType.DMA,
            pltpu.SemaphoreType.DMA,
            pltpu.SemaphoreType.DMA,
            pltpu.SemaphoreType.DMA((SENDS,)),
            pltpu.SemaphoreType.DMA((RECVS,)),
        ],
        compiler_params=pltpu.CompilerParams(
            collective_id=0, has_side_effects=True, vmem_limit_bytes=58 * 1024 * 1024
        ),
    )(inputs, w_query, w_key, w_value, rel_bias.T, d_out)
    gx, gwq, gwk, gwv, gb = pl.pallas_call(
        write_out,
        out_shape=(
            jax.ShapeDtypeStruct((512, 768), BF),
            jax.ShapeDtypeStruct((96, 384), F32),
            jax.ShapeDtypeStruct((96, 384), F32),
            jax.ShapeDtypeStruct((96, 384), F32),
            jax.ShapeDtypeStruct((6, 320), F32),
        ),
        in_specs=[vmem] * 3,
        out_specs=[any_spec] * 5,
        scratch_shapes=[pltpu.SemaphoreType.DMA((5,))],
        compiler_params=pltpu.CompilerParams(vmem_limit_bytes=4 * 1024 * 1024),
    )(gx, gw, gb)
    return gx, gwq, gwk, gwv, gb.T


def solution(mesh):
    torus = Mesh(mesh.devices.reshape(4, 4, 2, mesh.shape["tp"]), ("sp_0", "sp_1", "sp_2", "tp"))
    return jax.shard_map(
        local,
        mesh=torus,
        in_specs=(
            P(SP, "tp"),
            P(None, "tp"),
            P(None, "tp"),
            P(None, "tp"),
            P(None, "tp"),
            P(SP, "tp"),
        ),
        out_specs=(P(SP, "tp"), P(SP, "tp"), P(SP, "tp"), P(SP, "tp"), P(None, "tp")),
        check_vma=False,
    )
```
